256 devices in a mesh: dp: 4 (over y), kv: 32 (over z, x), tp: 2 (over core).
Axes of the slice: x: 4, y: 4, z: 8, core: 2. Of those that a mesh axis runs over, the one named last changes fastest.
Arguments:
- tokens: bfloat16 [1024, 4096], P('dp', ('kv', 'tp')), may hold values from -11.5 to 11.5, as said below
- gain_mix: float32 [4096], replicated, may hold values from 0.1 to 1.9
- gain_mlp: float32 [4096], replicated, may hold values from 0.1 to 1.9
- decay_rate: float32 [16], replicated, may hold values from 0.01 to 1
- w_query: bfloat16 [4096, 1024], P('kv', 'tp'), may hold values from -0.09375 to 0.09375
- w_key: bfloat16 [4096, 1024], P('kv', 'tp'), may hold values from -0.09375 to 0.09375
- w_value: bfloat16 [4096, 2048], P('kv', 'tp'), may hold values from -0.09375 to 0.09375
- w_gate: bfloat16 [4096, 2048], P('kv', 'tp'), may hold values from -0.09375 to 0.09375
- w_mix: bfloat16 [2048, 4096], P('tp', 'kv'), may hold values from -0.125 to 0.125
- w_up: bfloat16 [4096, 16384], P(None, ('kv', 'tp')), may hold values from -0.09375 to 0.09375
- w_down: bfloat16 [16384, 4096], P(('kv', 'tp')), may hold values from -0.125 to 0.125
- state: float32 [1024, 16, 64, 128], P(('dp', 'kv'), 'tp'), may hold values from -2 to 2
Outputs:
- result: bfloat16 [1024, 4096], P('dp', ('kv', 'tp'))
- new_state: float32 [1024, 16, 64, 128], P(('dp', 'kv'), 'tp')
The draws below stay inside these ranges and needn't reach their ends.
Inputs may be any that keep to these rules, and one draw needn't show every extreme that they name: `tokens`: feature scales differ across the features.
All inputs are finite; a program needn't handle non-finite values.
Results may differ from the reference program's by a relative error of at most 0.02.
Values may be sent and summed in bfloat16 or wider, within the bound.
No kernel may reach another device: no remote copies, remote signals or barrier semaphores. Data moves between devices by JAX's collectives and lax.ppermute only.
A program may use at most 64 MiB of HBM per device.

```python
import math
import jax
import jax.numpy as jnp
from jax import lax

D = 4096
HEADS = 16
DK = 64
DV = 128
FF = 16384
BATCH = 1024
N_TP = 2


def draw_tokens(key, part):
    col_scale = jnp.exp(jnp.linspace(jnp.log(0.35), jnp.log(2.8), D)).astype(jnp.float32)
    normal_part = jnp.clip(jax.random.normal(key, (BATCH, D), jnp.float32), -4.0, 4.0)
    values_out = normal_part * col_scale[None, :]
    return values_out.astype(jnp.bfloat16)


def spiked(array, stream_key, source, target, parts, factor):
    def block_of(dim):
        return (jnp.arange(array.shape[dim]) // (array.shape[dim] // parts)).reshape((-1,) + (1,) * (array.ndim - 1 - dim))

    near = jax.random.permutation(stream_key, parts)[block_of(target)]
    far = (block_of(target) + parts // 2) % parts
    return jnp.where((block_of(source) == near) | (block_of(source) == far), factor * array, array)


def block_scale(rng, shape, shards, least, largest):
    def one(position, parts):
        heights = jax.random.uniform(jax.random.fold_in(jax.random.fold_in(rng, 6), position), (parts,), jnp.float32, least / len(shards), largest / len(shards))
        return jnp.repeat(jnp.exp(heights), shape[position] // parts).reshape((-1,) + (1,) * (len(shape) - position - 1))

    gain = one(*shards[0])
    for cut in shards[1:]:
        gain = gain * one(*cut)
    return gain


def scatter_about(own_key, shape, deviation, bound, pieces=(), kind=jnp.bfloat16):
    loudness = block_scale(own_key, shape, pieces, -0.22, 0.18) if pieces else 1.0
    drawn = jax.random.normal(own_key, shape, jnp.float32) * deviation * loudness
    return jnp.minimum(jnp.maximum(drawn, -bound), bound).astype(kind)


def noise_with(own_key, shape, width, limit, pieces, heavy, dtype=jnp.bfloat16):
    entries = width * jax.random.normal(own_key, shape, jnp.float32)
    if pieces:
        entries = entries * block_scale(own_key, shape, pieces, -0.22, 0.18)
    return jnp.clip(spiked(entries, jax.random.fold_in(own_key, 3), *heavy), -limit, limit).astype(dtype)


def setup_inputs(seed: int = 0) -> dict:
    key_list = jax.random.split(jax.random.key(seed), 13)
    tokens = draw_tokens(jax.random.fold_in(key_list[12], 71), 0)
    gain_mix = jnp.clip(1.0 + 0.18 * jax.random.normal(key_list[1], (D,), jnp.float32), 0.1, 1.9)
    gain_mlp = jnp.clip(1.0 + 0.18 * jax.random.normal(key_list[2], (D,), jnp.float32), 0.1, 1.9)
    decay_rate = jnp.clip(jnp.exp(jax.random.uniform(key_list[3], (HEADS,), jnp.float32, math.log(0.01), math.log(1.0))), 0.01, 1.0)
    w_query = scatter_about(key_list[4], (D, HEADS * DK), D ** -0.5, 0.09375, ((0, 32), (1, 2)))
    w_key = scatter_about(key_list[5], (D, HEADS * DK), D ** -0.5, 0.09375, ((0, 32), (1, 2)))
    w_value = scatter_about(key_list[6], (D, HEADS * DV), D ** -0.5, 0.09375, ((0, 32), (1, 2)))
    w_gate = scatter_about(key_list[7], (D, HEADS * DV), D ** -0.5, 0.09375, ((0, 32), (1, 2)))
    w_mix = scatter_about(key_list[8], (HEADS * DV, D), (HEADS * DV) ** -0.5, 0.125, ((0, 2), (1, 32)))
    w_up = scatter_about(key_list[9], (D, FF), D ** -0.5, 0.09375, ((1, 64),))
    w_down = noise_with(key_list[10], (FF, D), FF ** -0.5, 0.125, ((0, 64),), (0, 1, 64, 4.0))
    state = scatter_about(key_list[11], (BATCH, HEADS, DK, DV), 0.3, 2.0, ((0, 128), (1, 2)), jnp.float32)
    return {"tokens": tokens, "gain_mix": gain_mix, "gain_mlp": gain_mlp, "decay_rate": decay_rate, "w_query": w_query, "w_key": w_key, "w_value": w_value, "w_gate": w_gate, "w_mix": w_mix, "w_up": w_up, "w_down": w_down, "state": state}


EPS = 1e-06

def reference(tokens, gain_mix, gain_mlp, decay_rate, w_query, w_key, w_value, w_gate, w_mix, w_up, w_down, state):
    batch = tokens.shape[0]
    inputs = tokens.astype(jnp.float32)
    first_scale = lax.rsqrt(lax.optimization_barrier(jnp.mean(inputs * inputs, axis=1, keepdims=True)) + EPS)
    normed = (inputs * first_scale * gain_mix).astype(jnp.bfloat16)
    query = jnp.dot(normed, w_query, preferred_element_type=jnp.float32).astype(jnp.bfloat16)
    keys = jnp.dot(normed, w_key, preferred_element_type=jnp.float32).astype(jnp.bfloat16)
    values = jnp.dot(normed, w_value, preferred_element_type=jnp.float32).astype(jnp.bfloat16)
    gates = jnp.dot(normed, w_gate, preferred_element_type=jnp.float32).astype(jnp.bfloat16)
    query_heads = query.astype(jnp.float32).reshape(batch, HEADS, DK)
    key_heads = keys.astype(jnp.float32).reshape(batch, HEADS, DK) * DK ** (-0.5)
    value_heads = values.astype(jnp.float32).reshape(batch, HEADS, DV)
    gate_heads = gates.astype(jnp.float32).reshape(batch, HEADS, DV)
    decay = jnp.exp(-decay_rate)[None, :, None, None]
    new_state = decay * state + key_heads[:, :, :, None] * value_heads[:, :, None, :]
    read = jnp.einsum('bhd,bhde->bhe', query_heads, new_state, precision=lax.Precision.HIGHEST)
    read = read * lax.rsqrt(lax.optimization_barrier(jnp.mean(read * read, axis=2, keepdims=True)) + EPS)
    heads_out = (jax.nn.silu(gate_heads) * read).reshape(batch, HEADS * DV).astype(jnp.bfloat16)
    group = HEADS * DV // N_TP
    mixed = jnp.zeros((batch, D), jnp.float32)
    for index in range(N_TP):
        product = jnp.dot(heads_out[:, index * group:(index + 1) * group], w_mix[index * group:(index + 1) * group], preferred_element_type=jnp.float32)
        rounded = lax.optimization_barrier(product.astype(jnp.bfloat16))
        mixed = mixed + rounded.astype(jnp.float32)
    resid = (inputs + mixed).astype(jnp.bfloat16)
    resid_f = resid.astype(jnp.float32)
    second_scale = lax.rsqrt(lax.optimization_barrier(jnp.mean(resid_f * resid_f, axis=1, keepdims=True)) + EPS)
    normed_mlp = (resid_f * second_scale * gain_mlp).astype(jnp.bfloat16)
    upper = jnp.dot(normed_mlp, w_up, preferred_element_type=jnp.float32)
    hidden = jnp.square(jax.nn.relu(upper)).astype(jnp.bfloat16)
    down = jnp.dot(hidden, w_down, preferred_element_type=jnp.float32)
    result = (resid_f + down).astype(jnp.bfloat16)
    return (result, new_state)
```

```python
import jax
import jax.numpy as jnp
from jax import lax
from jax.experimental import pallas as pl
from jax.experimental.pallas import tpu as pltpu
from jax.sharding import Mesh
from jax.sharding import PartitionSpec as P

KV = ("kv_0", "kv_1")
KV_TP = ("kv_0", "kv_1", "tp")
DP_KV = ("dp", "kv_0", "kv_1")

EPS = 1e-06
F32 = jnp.float32
BF16 = jnp.bfloat16
LANES = 128


def dot(a, b):
    return jnp.dot(a, b, preferred_element_type=F32)


def kernel_call(body, outs, *args, scratch=(), smem=(), flops=0, bytes_accessed=0):
    vmem = pl.BlockSpec(memory_space=pltpu.VMEM)
    in_smem = pl.BlockSpec(memory_space=pltpu.SMEM)
    return pl.pallas_call(
        body,
        out_shape=[jax.ShapeDtypeStruct(*o) for o in outs],
        in_specs=[in_smem if i in smem else vmem for i in range(len(args))],
        out_specs=[vmem] * len(outs),
        scratch_shapes=list(scratch),
        cost_estimate=pl.CostEstimate(
            flops=flops, bytes_accessed=bytes_accessed, transcendentals=0
        ),
    )(*args)


def swap_tp(x):
    return lax.ppermute(x, "tp", [(0, 1), (1, 0)])


def inputs_kernel(place, own, other, gain, w_query, w_key, w_value, w_gate, out, both_out):
    tp = place[0]
    first, second = own[...], other[...]
    both = jnp.where(
        tp == 0,
        jnp.concatenate([first, second], axis=1).astype(F32),
        jnp.concatenate([second, first], axis=1).astype(F32),
    )
    both_out[...] = both.astype(BF16)
    squares = jnp.sum(both * both, axis=1, keepdims=True)
    scaled = (both * gain[pl.ds(place[1], 1), :]).astype(BF16)
    start = 0
    for weight in (w_query, w_key, w_value, w_gate):
        width = weight.shape[1]
        out[:, start : start + width] = dot(scaled, weight[...]).astype(BF16)
        start += width
    high = squares.astype(BF16).astype(F32)
    low = squares - high
    lane = lax.broadcasted_iota(jnp.int32, (squares.shape[0], LANES), 1)
    out[:, start : start + LANES] = jnp.where(
        lane == 0, high, jnp.where(lane == 1, low, 0.0)
    ).astype(BF16)


def retention_kernel(parts, state, decay, new_state, heads_out, read_ref, *, model_width, sizes):
    seqs, heads, key_width, value_width = sizes
    peers = parts.shape[0]
    total = parts[0].astype(F32)
    for j in range(1, peers):
        total = total + parts[j].astype(F32)
    q_end = heads * key_width
    k_end = 2 * q_end
    v_end = k_end + heads * value_width
    g_end = v_end + heads * value_width
    row_total = total[:, g_end : g_end + 1] + total[:, g_end + 1 : g_end + 2]
    scale = lax.rsqrt(row_total / model_width + EPS)

    def rounded(x):
        return (x * scale).astype(BF16).astype(F32)

    query = rounded(total[:, :q_end])
    key = rounded(total[:, q_end:k_end]) * key_width ** (-0.5)
    value = rounded(total[:, k_end:v_end])
    gate = rounded(total[:, v_end:g_end])
    query_t = query.T
    key_t = key.T
    for b in range(seqs):
        for h in range(heads):
            rows = slice(h * key_width, (h + 1) * key_width)
            cols = slice(h * value_width, (h + 1) * value_width)
            old = state[b * heads + h]
            new = decay[h : h + 1, :] * old + key_t[rows, b : b + 1] * value[b : b + 1, cols]
            new_state[b * heads + h] = new
            read_ref[b : b + 1, cols] = jnp.sum(
                query_t[rows, b : b + 1] * new, axis=0, keepdims=True
            )
    for h in range(heads):
        cols = slice(h * value_width, (h + 1) * value_width)
        read = read_ref[:, cols]
        read = read * lax.rsqrt(jnp.mean(read * read, axis=1, keepdims=True) + EPS)
        g = gate[:, cols]
        done = (g / (1.0 + jnp.exp(-g)) * read).astype(BF16)
        for j in range(peers):
            heads_out[j, :, cols] = done


def mix_kernel(place, heads, w_mix, keep, send):
    tp = place[0]
    half = keep.shape[0]
    product = dot(heads[...], w_mix[...]).astype(BF16)
    top, bottom = product[:half], product[half:]
    keep[...] = jnp.where(tp == 0, top.astype(F32), bottom.astype(F32)).astype(BF16)
    send[...] = jnp.where(tp == 0, bottom.astype(F32), top.astype(F32)).astype(BF16)


def resid_kernel(place, both, keep, received, out):
    half = keep.shape[0]
    start = pl.multiple_of(place[0] * half, half)
    mixed = keep[...].astype(F32) + received[...].astype(F32)
    resid = (both[pl.ds(start, half), :].astype(F32) + mixed).astype(BF16)
    for j in range(out.shape[0]):
        out[j] = resid


def mixer_kernel(place, mine, other, gain, w_up, w_down, keep, send, resid, *, model_width):
    tp = place[0]
    peers, half, width = mine.shape
    hidden_width = w_up.shape[1]
    squares = jnp.zeros((2 * half, width), F32)
    upper = jnp.zeros((2 * half, hidden_width), F32)
    for j in range(0, peers, 2):
        pieces = []
        for i in (j, j + 1):
            block = jnp.concatenate([mine[i], other[i]], axis=0).astype(F32)
            squares = squares + block * block
            pieces.append((block * gain[i : i + 1, :]).astype(BF16))
        upper = upper + dot(
            jnp.concatenate(pieces, axis=1), w_up[j * width : (j + 2) * width, :]
        )
    scale = lax.rsqrt(jnp.sum(squares, axis=1, keepdims=True) / model_width + EPS)
    upper = jnp.maximum(upper * scale, 0.0)
    hidden = (upper * upper).astype(BF16)
    lane = lax.broadcasted_iota(jnp.int32, (half, width), 1)
    own = jnp.where(lane < width // 2, 0, 1) == tp

    for j in range(0, peers, 2):
        pair = dot(hidden, w_down[:, j * width : (j + 2) * width])
        for i in (j, j + 1):
            cols = slice((i - j) * width, (i - j + 1) * width)
            from_mine, from_other = pair[:half, cols], pair[half:, cols]
            keep[i] = jnp.where(own, from_mine, pltpu.roll(from_other, width // 2, 1))
            send[i] = jnp.where(own, pltpu.roll(from_mine, width // 2, 1), from_other).astype(BF16)
    spot = place[1]
    resid[...] = jnp.where(
        own,
        mine[spot].astype(F32),
        pltpu.roll(other[spot].astype(F32), width // 2, 1),
    )


def result_kernel(parts, resid, out):
    half, width = resid.shape
    total = parts[0].astype(F32)
    for j in range(1, parts.shape[0]):
        total = total + parts[j].astype(F32)
    total = resid[...] + total
    out[:half, :] = total[:, : width // 2].astype(BF16)
    out[half:, :] = pltpu.roll(total, width // 2, 1)[:, : width // 2].astype(BF16)


def per_device(
    tokens,
    gain_mix,
    gain_mlp,
    decay_rate,
    w_query,
    w_key,
    w_value,
    w_gate,
    w_mix,
    w_up,
    w_down,
    state,
):
    seqs, heads, key_width, value_width = state.shape
    rows, own_cols = tokens.shape
    half = rows // 2
    cols = 2 * own_cols
    peers = lax.axis_size(KV)
    model_width = cols * peers
    tp = lax.axis_index("tp")
    kv = lax.axis_index(KV)
    place = jnp.stack([tp, kv]).astype(jnp.int32)
    qkvg = sum(w.shape[1] for w in (w_query, w_key, w_value, w_gate))
    payload, both = kernel_call(
        inputs_kernel,
        [((rows, qkvg + LANES), BF16), ((rows, cols), BF16)],
        place,
        tokens,
        swap_tp(tokens),
        gain_mix.reshape(peers, cols),
        w_query,
        w_key,
        w_value,
        w_gate,
        smem=(0,),
    )
    parts = lax.all_to_all(
        payload.reshape(peers, seqs, qkvg + LANES), KV, 0, 0, tiled=True
    )
    rates = lax.dynamic_slice_in_dim(decay_rate, tp * heads, heads)
    decay = jnp.broadcast_to(jnp.exp(-rates)[:, None], (heads, value_width))

    def retention_body(*refs):
        retention_kernel(
            *refs, model_width=model_width, sizes=(seqs, heads, key_width, value_width)
        )

    new_state, heads_out = kernel_call(
        retention_body,
        [
            ((seqs * heads, key_width, value_width), F32),
            ((peers, seqs, heads * value_width), BF16),
        ],
        parts,
        state.reshape(seqs * heads, key_width, value_width),
        decay,
        scratch=[pltpu.VMEM((seqs, heads * value_width), F32)],
    )
    all_heads = lax.all_to_all(heads_out, KV, 0, 0, tiled=True)
    keep, send = kernel_call(
        mix_kernel,
        [((half, cols), BF16)] * 2,
        place,
        all_heads.reshape(rows, heads * value_width),
        w_mix,
        smem=(0,),
    )
    (resid,) = kernel_call(
        resid_kernel,
        [((peers, half, cols), BF16)],
        place,
        both,
        keep,
        swap_tp(send),
        smem=(0,),
    )
    mine = lax.all_to_all(resid, KV, 0, 0, tiled=True)
    other = swap_tp(mine)

    def mixer_body(*refs):
        mixer_kernel(*refs, model_width=model_width)

    keep, send, own_resid = kernel_call(
        mixer_body,
        [((peers, half, cols), F32), ((peers, half, cols), BF16), ((half, cols), F32)],
        place,
        mine,
        other,
        gain_mlp.reshape(peers, cols),
        w_up,
        w_down,
        smem=(0,),
    )
    chip_sum = (keep + swap_tp(send).astype(F32)).astype(BF16)
    parts = lax.all_to_all(chip_sum, KV, 0, 0, tiled=True)
    (result,) = kernel_call(result_kernel, [((rows, own_cols), BF16)], parts, own_resid)
    return (result, new_state.reshape(state.shape))


def solution(mesh):
    torus = Mesh(
        mesh.devices.reshape(mesh.shape["dp"], 8, 4, mesh.shape["tp"]), ("dp", "kv_0", "kv_1", "tp")
    )
    return jax.shard_map(
        per_device,
        mesh=torus,
        in_specs=(
            P("dp", KV_TP),
            P(),
            P(),
            P(),
            P(KV, "tp"),
            P(KV, "tp"),
            P(KV, "tp"),
            P(KV, "tp"),
            P("tp", KV),
            P(None, KV_TP),
            P(KV_TP, None),
            P(DP_KV, "tp", None, None),
        ),
        out_specs=(P("dp", KV_TP), P(DP_KV, "tp", None, None)),
        check_vma=False,
    )
```

```python
import jax
import jax.numpy as jnp
from jax import lax
from jax.experimental import pallas as pl
from jax.experimental.pallas import tpu as pltpu
from jax.sharding import Mesh
from jax.sharding import PartitionSpec as P

KV = ("kv_0", "kv_1")
KV_TP = ("kv_0", "kv_1", "tp")
DP_KV = ("dp", "kv_0", "kv_1")

EPS = 1e-06
F32 = jnp.float32
BF16 = jnp.bfloat16
LANES = 128


def dot(a, b):
    return jnp.dot(a, b, preferred_element_type=F32)


def kernel_call(body, outs, *args, scratch=(), smem=(), flops=0, bytes_accessed=0):
    vmem = pl.BlockSpec(memory_space=pltpu.VMEM)
    in_smem = pl.BlockSpec(memory_space=pltpu.SMEM)
    return pl.pallas_call(
        body,
        out_shape=[jax.ShapeDtypeStruct(*o) for o in outs],
        in_specs=[in_smem if i in smem else vmem for i in range(len(args))],
        out_specs=[vmem] * len(outs),
        scratch_shapes=list(scratch),
        compiler_params=pltpu.CompilerParams(vmem_limit_bytes=20 * 2**20),
        cost_estimate=pl.CostEstimate(
            flops=flops, bytes_accessed=bytes_accessed, transcendentals=0
        ),
    )(*args)


def swap_tp(x):
    return lax.ppermute(x, "tp", [(0, 1), (1, 0)])


def inputs_kernel(place, own, other, gain, w_query, w_key, w_value, w_gate, out, both_out):
    tp = place[0]
    first, second = own[...], other[...]
    both = jnp.where(
        tp == 0,
        jnp.concatenate([first, second], axis=1).astype(F32),
        jnp.concatenate([second, first], axis=1).astype(F32),
    )
    both_out[...] = both.astype(BF16)
    squares = jnp.sum(both * both, axis=1, keepdims=True)
    scaled = (both * gain[pl.ds(place[1], 1), :]).astype(BF16)
    start = 0
    for weight in (w_query, w_key, w_value, w_gate):
        width = weight.shape[1]
        out[:, start : start + width] = dot(scaled, weight[...]).astype(BF16)
        start += width
    high = squares.astype(BF16).astype(F32)
    low = squares - high
    lane = lax.broadcasted_iota(jnp.int32, (squares.shape[0], LANES), 1)
    out[:, start : start + LANES] = jnp.where(
        lane == 0, high, jnp.where(lane == 1, low, 0.0)
    ).astype(BF16)


def retention_kernel(parts, state, decay, new_state, heads_out, read_ref, *, model_width, sizes):
    seqs, heads, key_width, value_width = sizes
    peers = parts.shape[0]
    total = parts[0].astype(F32)
    for j in range(1, peers):
        total = total + parts[j].astype(F32)
    q_end = heads * key_width
    k_end = 2 * q_end
    v_end = k_end + heads * value_width
    g_end = v_end + heads * value_width
    row_total = total[:, g_end : g_end + 1] + total[:, g_end + 1 : g_end + 2]
    scale = lax.rsqrt(row_total / model_width + EPS)

    def rounded(x):
        return (x * scale).astype(BF16).astype(F32)

    query = rounded(total[:, :q_end])
    key = rounded(total[:, q_end:k_end]) * key_width ** (-0.5)
    value = rounded(total[:, k_end:v_end])
    gate = rounded(total[:, v_end:g_end])
    query_t = query.T
    key_t = key.T
    for b in range(seqs):
        for h in range(heads):
            rows = slice(h * key_width, (h + 1) * key_width)
            cols = slice(h * value_width, (h + 1) * value_width)
            old = state[b * heads + h]
            new = decay[h : h + 1, :] * old + key_t[rows, b : b + 1] * value[b : b + 1, cols]
            new_state[b * heads + h] = new
            read_ref[b : b + 1, cols] = jnp.sum(
                query_t[rows, b : b + 1] * new, axis=0, keepdims=True
            )
    for h in range(heads):
        cols = slice(h * value_width, (h + 1) * value_width)
        read = read_ref[:, cols]
        read = read * lax.rsqrt(jnp.mean(read * read, axis=1, keepdims=True) + EPS)
        g = gate[:, cols]
        done = (g / (1.0 + jnp.exp(-g)) * read).astype(BF16)
        for j in range(peers):
            heads_out[j, :, cols] = done


def mix_kernel(place, heads, w_mix, keep, send):
    tp = place[0]
    half = keep.shape[0]
    product = dot(heads[...], w_mix[...]).astype(BF16)
    top, bottom = product[:half], product[half:]
    keep[...] = jnp.where(tp == 0, top.astype(F32), bottom.astype(F32)).astype(BF16)
    send[...] = jnp.where(tp == 0, bottom.astype(F32), top.astype(F32)).astype(BF16)


def resid_kernel(place, both, keep, received, out):
    half = keep.shape[0]
    start = pl.multiple_of(place[0] * half, half)
    mixed = keep[...].astype(F32) + received[...].astype(F32)
    resid = (both[pl.ds(start, half), :].astype(F32) + mixed).astype(BF16)
    for j in range(out.shape[0]):
        out[j] = resid


def mixer_kernel(place, mine, other, gain, w_up, w_down, keep, send, resid, *, model_width):
    tp = place[0]
    peers, half, width = mine.shape
    hidden_width = w_up.shape[1]
    squares = jnp.zeros((2 * half, width), F32)
    upper = jnp.zeros((2 * half, hidden_width), F32)
    for j in range(0, peers, 2):
        pieces = []
        for i in (j, j + 1):
            block = jnp.concatenate([mine[i], other[i]], axis=0).astype(F32)
            squares = squares + block * block
            pieces.append((block * gain[i : i + 1, :]).astype(BF16))
        upper = upper + dot(
            jnp.concatenate(pieces, axis=1), w_up[j * width : (j + 2) * width, :]
        )
    scale = lax.rsqrt(jnp.sum(squares, axis=1, keepdims=True) / model_width + EPS)
    upper = jnp.maximum(upper * scale, 0.0)
    hidden = (upper * upper).astype(BF16)
    lane = lax.broadcasted_iota(jnp.int32, (half, width), 1)
    own = jnp.where(lane < width // 2, 0, 1) == tp

    for j in range(0, peers, 2):
        pair = dot(hidden, w_down[:, j * width : (j + 2) * width])
        for i in (j, j + 1):
            cols = slice((i - j) * width, (i - j + 1) * width)
            from_mine, from_other = pair[:half, cols], pair[half:, cols]
            keep[i] = jnp.where(own, from_mine, pltpu.roll(from_other, width // 2, 1))
            send[i] = jnp.where(own, pltpu.roll(from_mine, width // 2, 1), from_other).astype(BF16)
    spot = place[1]
    resid[...] = jnp.where(
        own,
        mine[spot].astype(F32),
        pltpu.roll(other[spot].astype(F32), width // 2, 1),
    )


def result_kernel(parts, resid, out):
    half, width = resid.shape
    total = parts[0].astype(F32)
    for j in range(1, parts.shape[0]):
        total = total + parts[j].astype(F32)
    total = resid[...] + total
    out[:half, :] = total[:, : width // 2].astype(BF16)
    out[half:, :] = pltpu.roll(total, width // 2, 1)[:, : width // 2].astype(BF16)


def per_device(
    tokens,
    gain_mix,
    gain_mlp,
    decay_rate,
    w_query,
    w_key,
    w_value,
    w_gate,
    w_mix,
    w_up,
    w_down,
    state,
):
    seqs, heads, key_width, value_width = state.shape
    rows, own_cols = tokens.shape
    half = rows // 2
    cols = 2 * own_cols
    peers = lax.axis_size(KV)
    model_width = cols * peers
    tp = lax.axis_index("tp")
    kv = lax.axis_index(KV)
    place = jnp.stack([tp, kv]).astype(jnp.int32)
    qkvg = sum(w.shape[1] for w in (w_query, w_key, w_value, w_gate))
    payload, both = kernel_call(
        inputs_kernel,
        [((rows, qkvg + LANES), BF16), ((rows, cols), BF16)],
        place,
        tokens,
        swap_tp(tokens),
        gain_mix.reshape(peers, cols),
        w_query,
        w_key,
        w_value,
        w_gate,
        smem=(0,),
    )
    parts = lax.all_to_all(
        payload.reshape(peers, seqs, qkvg + LANES), KV, 0, 0, tiled=True
    )
    rates = lax.dynamic_slice_in_dim(decay_rate, tp * heads, heads)
    decay = jnp.broadcast_to(jnp.exp(-rates)[:, None], (heads, value_width))

    def retention_body(*refs):
        retention_kernel(
            *refs, model_width=model_width, sizes=(seqs, heads, key_width, value_width)
        )

    new_state, heads_out = kernel_call(
        retention_body,
        [
            ((seqs * heads, key_width, value_width), F32),
            ((peers, seqs, heads * value_width), BF16),
        ],
        parts,
        state.reshape(seqs * heads, key_width, value_width),
        decay,
        scratch=[pltpu.VMEM((seqs, heads * value_width), F32)],
    )
    all_heads = lax.all_to_all(heads_out, KV, 0, 0, tiled=True)
    keep, send = kernel_call(
        mix_kernel,
        [((half, cols), BF16)] * 2,
        place,
        all_heads.reshape(rows, heads * value_width),
        w_mix,
        smem=(0,),
    )
    (resid,) = kernel_call(
        resid_kernel,
        [((peers, half, cols), BF16)],
        place,
        both,
        keep,
        swap_tp(send),
        smem=(0,),
    )
    mine = lax.all_to_all(resid, KV, 0, 0, tiled=True)
    other = swap_tp(mine)

    def mixer_body(*refs):
        mixer_kernel(*refs, model_width=model_width)

    keep, send, own_resid = kernel_call(
        mixer_body,
        [((peers, half, cols), F32), ((peers, half, cols), BF16), ((half, cols), F32)],
        place,
        mine,
        other,
        gain_mlp.reshape(peers, cols),
        w_up,
        w_down,
        smem=(0,),
    )
    chip_sum = (keep + swap_tp(send).astype(F32)).astype(BF16)
    parts = lax.all_to_all(chip_sum, KV, 0, 0, tiled=True)
    (result,) = kernel_call(result_kernel, [((rows, own_cols), BF16)], parts, own_resid)
    return (result, new_state.reshape(state.shape))


def solution(mesh):
    torus = Mesh(
        mesh.devices.reshape(mesh.shape["dp"], 8, 4, mesh.shape["tp"]), ("dp", "kv_0", "kv_1", "tp")
    )
    return jax.shard_map(
        per_device,
        mesh=torus,
        in_specs=(
            P("dp", KV_TP),
            P(),
            P(),
            P(),
            P(KV, "tp"),
            P(KV, "tp"),
            P(KV, "tp"),
            P(KV, "tp"),
            P("tp", KV),
            P(None, KV_TP),
            P(KV_TP, None),
            P(DP_KV, "tp", None, None),
        ),
        out_specs=(P("dp", KV_TP), P(DP_KV, "tp", None, None)),
        check_vma=False,
    )
```

```python
import jax
import jax.numpy as jnp
from jax import lax
from jax.experimental import pallas as pl
from jax.experimental.pallas import tpu as pltpu
from jax.sharding import Mesh
from jax.sharding import PartitionSpec as P

KV = ("kv_0", "kv_1")
KV_TP = ("kv_0", "kv_1", "tp")
DP_KV = ("dp", "kv_0", "kv_1")

EPS = 1e-06
F32 = jnp.float32
BF16 = jnp.bfloat16
LANES = 128


def dot(a, b):
    return jnp.dot(a, b, preferred_element_type=F32)


def kernel_call(body, outs, *args, scratch=(), hbm=(), flops=0, bytes_accessed=0):
    vmem = pl.BlockSpec(memory_space=pltpu.VMEM)
    in_hbm = pl.BlockSpec(memory_space=pltpu.HBM)
    return pl.pallas_call(
        body,
        out_shape=[jax.ShapeDtypeStruct(*o) for o in outs],
        in_specs=[in_hbm if i in hbm else vmem for i in range(len(args))],
        out_specs=[vmem] * len(outs),
        scratch_shapes=list(scratch),
        compiler_params=pltpu.CompilerParams(vmem_limit_bytes=20 * 2**20),
        cost_estimate=pl.CostEstimate(
            flops=flops, bytes_accessed=bytes_accessed, transcendentals=0
        ),
    )(*args)


def swap_tp(x):
    return lax.ppermute(x, "tp", [(0, 1), (1, 0)])


def ring_sizes():
    return lax.axis_size("kv_0"), lax.axis_size("kv_1")


def parity_order(z_size, x_size):
    return [
        (2 * zr + zb) * x_size + 2 * xr + xb
        for zb in range(2)
        for xb in range(2)
        for zr in range(z_size // 2)
        for xr in range(x_size // 2)
    ]


def square_groups(z_size, x_size):
    groups = []
    for tp in range(2):
        for zs in range(z_size // 2):
            for xs in range(x_size // 2):
                at_z = {z % 2: z for z in ((2 * zs + tp + i) % z_size for i in range(2))}
                at_x = {x % 2: x for x in ((2 * xs + tp + i) % x_size for i in range(2))}
                groups.append(
                    [
                        (at_z[zb] * x_size + at_x[xb]) * 2 + tp
                        for zb in range(2)
                        for xb in range(2)
                    ]
                )
    return groups


def parity_groups(z_size, x_size):
    order = parity_order(z_size, x_size)
    count = len(order) // 4
    return [
        [kv * 2 + tp for kv in order[c * count : (c + 1) * count]]
        for tp in range(2)
        for c in range(4)
    ]


def in_groups(x, groups):
    return lax.all_to_all(x, KV_TP, 0, 0, axis_index_groups=groups, tiled=True)


def sum_at_owner(parts):
    sizes = ring_sizes()
    peers, *rest = parts.shape
    near = in_groups(parts.reshape(4, peers // 4, *rest), square_groups(*sizes))
    total = near.reshape(4, peers // 4, *rest).astype(F32).sum(axis=0).astype(BF16)
    return in_groups(total, parity_groups(*sizes))


def gathered(copies):
    sizes = ring_sizes()
    count, *rest = copies.shape
    far = in_groups(copies, parity_groups(*sizes))
    near = in_groups(jnp.broadcast_to(far[None], (4, count, *rest)), square_groups(*sizes))
    return near.reshape(4 * count, *rest)


def inputs_kernel(
    other, own, gain, w_query, w_key, w_value, w_gate, out, both_out, *scratch, order
):
    sources = (own, gain, w_query, w_key, w_value, w_gate)
    held, sem = scratch[:-1], scratch[-1]
    copies = [
        pltpu.make_async_copy(source, dest, sem.at[i])
        for i, (source, dest) in enumerate(zip(sources, held, strict=True))
    ]
    for copy in copies:
        copy.start()
    tp = lax.axis_index("tp")
    kv = lax.axis_index(KV)
    copies[0].wait()
    first, second = held[0][...].astype(F32), other[...].astype(F32)
    both = jnp.where(
        tp == 0,
        jnp.concatenate([first, second], axis=0),
        jnp.concatenate([second, first], axis=0),
    ).T
    both_out[...] = both.astype(BF16)
    seqs = both.shape[0] // len(order)
    both = jnp.concatenate([both[i * seqs : (i + 1) * seqs] for i in order], axis=0)
    squares = jnp.sum(both * both, axis=1, keepdims=True)
    high = squares.astype(BF16).astype(F32)
    low = squares - high
    lane = lax.broadcasted_iota(jnp.int32, (squares.shape[0], LANES), 1)
    copies[1].wait()
    scaled = (both * held[1][pl.ds(kv, 1), :]).astype(BF16)
    start = 0
    for weight, copy in zip(held[2:], copies[2:], strict=True):
        copy.wait()
        width = weight.shape[1]
        out[:, start : start + width] = dot(scaled, weight[...]).astype(BF16)
        start += width
    out[:, start : start + LANES] = jnp.where(
        lane == 0, high, jnp.where(lane == 1, low, 0.0)
    ).astype(BF16)


def decay_kernel(state, rates, out):
    heads = rates.shape[0]
    decay = jnp.exp(-rates[...])
    for i in range(out.shape[0]):
        h = i % heads
        out[i] = decay[h : h + 1, :] * state[i]


def retention_kernel(parts, decayed, new_state, heads_out, read_ref, *, model_width, sizes):
    seqs, heads, key_width, value_width = sizes
    total = parts[0].astype(F32)
    for j in range(1, parts.shape[0]):
        total = total + parts[j].astype(F32)
    q_end = heads * key_width
    k_end = 2 * q_end
    v_end = k_end + heads * value_width
    g_end = v_end + heads * value_width
    row_total = total[:, g_end : g_end + 1] + total[:, g_end + 1 : g_end + 2]
    scale = lax.rsqrt(row_total / model_width + EPS)

    def rounded(x):
        return (x * scale).astype(BF16).astype(F32)

    query = rounded(total[:, :q_end])
    key = rounded(total[:, q_end:k_end]) * key_width ** (-0.5)
    value = rounded(total[:, k_end:v_end])
    gate = rounded(total[:, v_end:g_end])
    query_t = query.T
    key_t = key.T
    for b in range(seqs):
        for h in range(heads):
            rows = slice(h * key_width, (h + 1) * key_width)
            cols = slice(h * value_width, (h + 1) * value_width)
            new = decayed[b * heads + h] + key_t[rows, b : b + 1] * value[b : b + 1, cols]
            new_state[b * heads + h] = new
            read_ref[b : b + 1, cols] = jnp.sum(
                query_t[rows, b : b + 1] * new, axis=0, keepdims=True
            )
    for h in range(heads):
        cols = slice(h * value_width, (h + 1) * value_width)
        read = read_ref[:, cols]
        read = read * lax.rsqrt(jnp.mean(read * read, axis=1, keepdims=True) + EPS)
        g = gate[:, cols]
        done = (g / (1.0 + jnp.exp(-g)) * read).astype(BF16)
        for j in range(heads_out.shape[0]):
            heads_out[j, :, cols] = done


def mix_kernel(heads, w_mix, keep, send):
    tp = lax.axis_index("tp")
    half = keep.shape[0]
    product = dot(heads[...], w_mix[...]).astype(BF16)
    top, bottom = product[:half], product[half:]
    keep[...] = jnp.where(tp == 0, top.astype(F32), bottom.astype(F32)).astype(BF16)
    send[...] = jnp.where(tp == 0, bottom.astype(F32), top.astype(F32)).astype(BF16)


def resid_kernel(both, keep, received, out):
    half = keep.shape[0]
    start = pl.multiple_of(lax.axis_index("tp") * half, half)
    mixed = keep[...].astype(F32) + received[...].astype(F32)
    resid = (both[pl.ds(start, half), :].astype(F32) + mixed).astype(BF16)
    for j in range(out.shape[0]):
        out[j] = resid


def mixer_kernel(mine, other, gain, w_up, w_down, keep, send, resid, *, model_width, order):
    tp = lax.axis_index("tp")
    kv = lax.axis_index(KV)
    peers, half, width = mine.shape
    hidden_width = w_up.shape[1]
    lane = lax.broadcasted_iota(jnp.int32, (half, width), 1)
    own = jnp.where(lane < width // 2, 0, 1) == tp
    squares = jnp.zeros((2 * half, width), F32)
    upper = jnp.zeros((2 * half, hidden_width), F32)
    own_resid = jnp.zeros((half, width), F32)
    for j in range(0, peers, 2):
        pieces = []
        for i in (j, j + 1):
            block = jnp.concatenate([mine[i], other[i]], axis=0).astype(F32)
            squares = squares + block * block
            pieces.append((block * gain[order[i] : order[i] + 1, :]).astype(BF16))
            place = jnp.where(kv == order[i], 1, 0)
            resid_here = jnp.where(
                own, block[:half], pltpu.roll(block[half:], width // 2, 1)
            )
            own_resid = jnp.where(place == 1, resid_here, own_resid)
        weights = [w_up[order[i] * width : (order[i] + 1) * width, :] for i in (j, j + 1)]
        upper = upper + dot(
            jnp.concatenate(pieces, axis=1), jnp.concatenate(weights, axis=0)
        )
    resid[...] = own_resid
    scale = lax.rsqrt(jnp.sum(squares, axis=1, keepdims=True) / model_width + EPS)
    upper = jnp.maximum(upper * scale, 0.0)
    hidden = (upper * upper).astype(BF16)
    for j in range(0, peers, 2):
        weights = [w_down[:, order[i] * width : (order[i] + 1) * width] for i in (j, j + 1)]
        pair = dot(hidden, jnp.concatenate(weights, axis=1))
        for i in (j, j + 1):
            cols = slice((i - j) * width, (i - j + 1) * width)
            from_mine, from_other = pair[:half, cols], pair[half:, cols]
            keep[i] = jnp.where(own, from_mine, pltpu.roll(from_other, width // 2, 1))
            send[i] = jnp.where(own, pltpu.roll(from_mine, width // 2, 1), from_other).astype(BF16)


def result_kernel(parts, resid, out):
    half, width = resid.shape
    total = parts[0].astype(F32)
    for j in range(1, parts.shape[0]):
        total = total + parts[j].astype(F32)
    total = (resid[...] + total).T
    out[:, :half] = total[: width // 2].astype(BF16)
    out[:, half:] = total[width // 2 :].astype(BF16)


def per_device(
    tokens,
    gain_mix,
    gain_mlp,
    decay_rate,
    w_query,
    w_key,
    w_value,
    w_gate,
    w_mix,
    w_up,
    w_down,
    state,
):
    seqs, heads, key_width, value_width = state.shape
    rows, own_cols = tokens.shape
    half = rows // 2
    cols = 2 * own_cols
    peers = lax.axis_size(KV)
    model_width = cols * peers
    order = parity_order(*ring_sizes())
    qkvg = sum(w.shape[1] for w in (w_query, w_key, w_value, w_gate))
    tokens_t = tokens.T

    def inputs_body(*refs):
        inputs_kernel(*refs, order=order)

    sources = [
        pltpu.with_memory_space_constraint(x, pltpu.HBM)
        for x in (tokens_t, gain_mix.reshape(peers, cols), w_query, w_key, w_value, w_gate)
    ]
    payload, both = kernel_call(
        inputs_body,
        [((rows, qkvg + LANES), BF16), ((rows, cols), BF16)],
        swap_tp(tokens_t),
        *sources,
        hbm=range(1, 7),
        scratch=[
            *(pltpu.VMEM(s.shape, s.dtype) for s in sources),
            pltpu.SemaphoreType.DMA((len(sources),)),
        ],
    )
    parts = sum_at_owner(payload.reshape(peers, seqs, qkvg + LANES))
    rates = lax.dynamic_slice_in_dim(decay_rate, lax.axis_index("tp") * heads, heads)
    (decayed,) = kernel_call(
        decay_kernel,
        [((seqs * heads, key_width, value_width), F32)],
        state.reshape(seqs * heads, key_width, value_width),
        jnp.broadcast_to(rates[:, None], (heads, value_width)),
        flops=10**7,
        bytes_accessed=2**23,
    )

    def retention_body(*refs):
        retention_kernel(
            *refs, model_width=model_width, sizes=(seqs, heads, key_width, value_width)
        )

    new_state, heads_out = kernel_call(
        retention_body,
        [
            ((seqs * heads, key_width, value_width), F32),
            ((peers, seqs, heads * value_width), BF16),
        ],
        parts,
        decayed,
        scratch=[pltpu.VMEM((seqs, heads * value_width), F32)],
    )
    all_heads = lax.all_to_all(heads_out, KV, 0, 0, tiled=True)
    keep, send = kernel_call(
        mix_kernel,
        [((half, cols), BF16)] * 2,
        all_heads.reshape(rows, heads * value_width),
        w_mix,
    )
    (resid,) = kernel_call(
        resid_kernel, [((peers // 4, half, cols), BF16)], both, keep, swap_tp(send)
    )
    mine = gathered(resid)
    other = swap_tp(mine)

    def mixer_body(*refs):
        mixer_kernel(*refs, model_width=model_width, order=order)

    keep, send, own_resid = kernel_call(
        mixer_body,
        [((peers, half, cols), F32), ((peers, half, cols), BF16), ((half, cols), F32)],
        mine,
        other,
        gain_mlp.reshape(peers, cols),
        w_up,
        w_down,
    )
    chip_sum = (keep + swap_tp(send).astype(F32)).astype(BF16)
    parts = sum_at_owner(chip_sum)
    (result_t,) = kernel_call(result_kernel, [((own_cols, rows), BF16)], parts, own_resid)
    return (result_t.T, new_state.reshape(state.shape))


def solution(mesh):
    torus = Mesh(
        mesh.devices.reshape(mesh.shape["dp"], 8, 4, mesh.shape["tp"]), ("dp", "kv_0", "kv_1", "tp")
    )
    return jax.shard_map(
        per_device,
        mesh=torus,
        in_specs=(
            P("dp", KV_TP),
            P(),
            P(),
            P(),
            P(KV, "tp"),
            P(KV, "tp"),
            P(KV, "tp"),
            P(KV, "tp"),
            P("tp", KV),
            P(None, KV_TP),
            P(KV_TP, None),
            P(DP_KV, "tp", None, None),
        ),
        out_specs=(P("dp", KV_TP), P(DP_KV, "tp", None, None)),
        check_vma=False,
    )
```

```python
import jax
import jax.numpy as jnp
from jax import lax
from jax.experimental import pallas as pl
from jax.experimental.pallas import tpu as pltpu
from jax.sharding import Mesh
from jax.sharding import PartitionSpec as P

KV = ("kv_0", "kv_1")
KV_TP = ("kv_0", "kv_1", "tp")
DP_KV = ("dp", "kv_0", "kv_1")

EPS = 1e-06
F32 = jnp.float32
BF16 = jnp.bfloat16
LANES = 128


def dot(a, b):
    return jnp.dot(a, b, preferred_element_type=F32)


def kernel_call(body, outs, *args, scratch=(), hbm=(), flops=0, bytes_accessed=0):
    vmem = pl.BlockSpec(memory_space=pltpu.VMEM)
    in_hbm = pl.BlockSpec(memory_space=pltpu.HBM)
    return pl.pallas_call(
        body,
        out_shape=[jax.ShapeDtypeStruct(*o) for o in outs],
        in_specs=[in_hbm if i in hbm else vmem for i in range(len(args))],
        out_specs=[vmem] * len(outs),
        scratch_shapes=list(scratch),
        compiler_params=pltpu.CompilerParams(vmem_limit_bytes=20 * 2**20),
        cost_estimate=pl.CostEstimate(
            flops=flops, bytes_accessed=bytes_accessed, transcendentals=0
        ),
    )(*args)


def swap_tp(x):
    return lax.ppermute(x, "tp", [(0, 1), (1, 0)])


def ring_sizes():
    return lax.axis_size("kv_0"), lax.axis_size("kv_1")


def own_class():
    return 2 * (lax.axis_index("kv_0") % 2) + lax.axis_index("kv_1") % 2


def members(z_size, x_size):
    return [(zr, xr) for zr in range(z_size // 2) for xr in range(x_size // 2)]


def member_kv(member, which, x_size):
    return (2 * member[0] + which // 2) * x_size + 2 * member[1] + which % 2


def class_groups():
    z_size, x_size = ring_sizes()
    return [
        [member_kv(m, c, x_size) * 2 + tp for m in members(z_size, x_size)]
        for tp in range(2)
        for c in range(4)
    ]


def to_neighbour(x, place):
    z_size, x_size = ring_sizes()

    def across(position, tp, size):
        return (position + (1 if position % 2 == tp else -1)) % size

    pairs = []
    for z in range(z_size):
        for x_ in range(x_size):
            for tp in range(2):
                to_z = across(z, tp, z_size) if place & 2 else z
                to_x = across(x_, tp, x_size) if place & 1 else x_
                pairs.append(((z * x_size + x_) * 2 + tp, (to_z * x_size + to_x) * 2 + tp))
    return lax.ppermute(x, KV_TP, pairs)


def in_class(x):
    return lax.all_to_all(x, KV_TP, 0, 0, axis_index_groups=class_groups(), tiled=True)


PLACES = (3, 1, 2)


def sum_at_owner(parts):
    arrived = {place: to_neighbour(parts[place], place) for place in PLACES}
    total = parts[0].astype(F32)
    for place in PLACES:
        total = total + arrived[place].astype(F32)
    return in_class(total.astype(BF16))


def gathered(copies):
    far = in_class(copies)
    arrived = {place: to_neighbour(far, place) for place in PLACES}
    return [far, *(arrived[place] for place in (1, 2, 3))]


def inputs_kernel(
    other, own, gain, w_query, w_key, w_value, w_gate, *rest, sizes
):
    outs, both_out, scratch = rest[:4], rest[4], rest[5:]
    sources = (own, gain, w_query, w_key, w_value, w_gate)
    held, by_class, sem = scratch[:-2], scratch[-2], scratch[-1]
    copies = [
        pltpu.make_async_copy(source, dest, sem.at[i])
        for i, (source, dest) in enumerate(zip(sources, held, strict=True))
    ]
    for copy in copies:
        copy.start()
    tp = lax.axis_index("tp")
    kv = lax.axis_index(KV)
    copies[0].wait()
    first, second = held[0][...].astype(F32), other[...].astype(F32)
    both = jnp.where(
        tp == 0,
        jnp.concatenate([first, second], axis=0),
        jnp.concatenate([second, first], axis=0),
    ).T
    both_out[...] = both.astype(BF16)
    seqs = both.shape[0] // (sizes[0] * sizes[1])
    for c in range(4):
        kvs = [member_kv(m, c, sizes[1]) for m in members(*sizes)]
        by_class[c] = jnp.concatenate([both[i * seqs : (i + 1) * seqs] for i in kvs], axis=0)
    both = jnp.concatenate([by_class[own_class() ^ place] for place in range(4)], axis=0)
    squares = jnp.sum(both * both, axis=1, keepdims=True)
    high = squares.astype(BF16).astype(F32)
    low = squares - high
    lane = lax.broadcasted_iota(jnp.int32, (squares.shape[0], LANES), 1)
    copies[1].wait()
    scaled = (both * held[1][pl.ds(kv, 1), :]).astype(BF16)
    start = 0
    for weight, copy in zip(held[2:], copies[2:], strict=True):
        copy.wait()
        width = weight.shape[1]
        product = dot(scaled, weight[...]).astype(BF16)
        for place, out in enumerate(outs):
            count = out.shape[0]
            out[:, start : start + width] = product[place * count : (place + 1) * count]
        start += width
    totals = jnp.where(lane == 0, high, jnp.where(lane == 1, low, 0.0)).astype(BF16)
    for place, out in enumerate(outs):
        count = out.shape[0]
        out[:, start : start + LANES] = totals[place * count : (place + 1) * count]


def decay_kernel(state, rates, out):
    heads = rates.shape[0]
    decay = jnp.exp(-rates[...])
    for i in range(out.shape[0]):
        h = i % heads
        out[i] = decay[h : h + 1, :] * state[i]


def retention_kernel(parts, decayed, new_state, heads_out, read_ref, *, model_width, sizes):
    seqs, heads, key_width, value_width = sizes
    total = parts[0].astype(F32)
    for j in range(1, parts.shape[0]):
        total = total + parts[j].astype(F32)
    q_end = heads * key_width
    k_end = 2 * q_end
    v_end = k_end + heads * value_width
    g_end = v_end + heads * value_width
    row_total = total[:, g_end : g_end + 1] + total[:, g_end + 1 : g_end + 2]
    scale = lax.rsqrt(row_total / model_width + EPS)

    def rounded(x):
        return (x * scale).astype(BF16).astype(F32)

    query = rounded(total[:, :q_end])
    key = rounded(total[:, q_end:k_end]) * key_width ** (-0.5)
    value = rounded(total[:, k_end:v_end])
    gate = rounded(total[:, v_end:g_end])
    query_t = query.T
    key_t = key.T
    for b in range(seqs):
        for h in range(heads):
            rows = slice(h * key_width, (h + 1) * key_width)
            cols = slice(h * value_width, (h + 1) * value_width)
            new = decayed[b * heads + h] + key_t[rows, b : b + 1] * value[b : b + 1, cols]
            new_state[b * heads + h] = new
            read_ref[b : b + 1, cols] = jnp.sum(
                query_t[rows, b : b + 1] * new, axis=0, keepdims=True
            )
    for h in range(heads):
        cols = slice(h * value_width, (h + 1) * value_width)
        read = read_ref[:, cols]
        read = read * lax.rsqrt(jnp.mean(read * read, axis=1, keepdims=True) + EPS)
        g = gate[:, cols]
        done = (g / (1.0 + jnp.exp(-g)) * read).astype(BF16)
        for j in range(heads_out.shape[0]):
            heads_out[j, :, cols] = done


def mix_kernel(*refs, sizes):
    heads, w_mix, keep, send, product = refs[:4], *refs[4:]
    tp = lax.axis_index("tp")
    seqs = heads[0].shape[0] // len(members(*sizes))
    for place in range(4):
        piece = dot(heads[place][...], w_mix[...])
        for i, m in enumerate(members(*sizes)):
            kv = member_kv(m, own_class() ^ place, sizes[1])
            product[pl.ds(pl.multiple_of(kv * seqs, seqs), seqs), :] = piece[
                i * seqs : (i + 1) * seqs
            ]
    half = keep.shape[0]
    keep[...] = product[pl.ds(pl.multiple_of(tp * half, half), half), :].astype(BF16)
    send[...] = product[pl.ds(pl.multiple_of((1 - tp) * half, half), half), :].astype(BF16)


def resid_kernel(both, keep, received, out):
    half = keep.shape[0]
    start = pl.multiple_of(lax.axis_index("tp") * half, half)
    mixed = keep[...].astype(F32) + received[...].astype(F32)
    resid = (both[pl.ds(start, half), :].astype(F32) + mixed).astype(BF16)
    for j in range(out.shape[0]):
        out[j] = resid


def mixer_kernel(*refs, model_width, sizes):
    mine, other, (gain, w_up, w_down), refs = refs[:4], refs[4:8], refs[8:11], refs[11:]
    keep, send, resid = refs[:4], refs[4:8], refs[8]
    tp = lax.axis_index("tp")
    kv_own = lax.axis_index(KV)
    count, half, width = mine[0].shape
    hidden_width = w_up.shape[1]
    lane = lax.broadcasted_iota(jnp.int32, (half, width), 1)
    own = jnp.where(lane < width // 2, 0, 1) == tp
    squares = jnp.zeros((2 * half, width), F32)
    upper = jnp.zeros((2 * half, hidden_width), F32)

    def kv_at(place, i):
        return member_kv(members(*sizes)[i], own_class() ^ place, sizes[1])

    for place in range(4):
        for j in range(0, count, 2):
            pieces, weights = [], []
            for i in (j, j + 1):
                kv = kv_at(place, i)
                block = jnp.concatenate([mine[place][i], other[place][i]], axis=0).astype(F32)
                squares = squares + block * block
                pieces.append((block * gain[pl.ds(kv, 1), :]).astype(BF16))
                weights.append(w_up[pl.ds(pl.multiple_of(kv * width, width), width), :])
            upper = upper + dot(
                jnp.concatenate(pieces, axis=1), jnp.concatenate(weights, axis=0)
            )
    spot = (kv_own // sizes[1] // 2) * (sizes[1] // 2) + kv_own % sizes[1] // 2
    resid[...] = jnp.where(
        own,
        mine[0][spot].astype(F32),
        pltpu.roll(other[0][spot].astype(F32), width // 2, 1),
    )
    scale = lax.rsqrt(jnp.sum(squares, axis=1, keepdims=True) / model_width + EPS)
    upper = jnp.maximum(upper * scale, 0.0)
    hidden = (upper * upper).astype(BF16)
    for place in (3, 1, 2, 0):
        for j in range(0, count, 2):
            weights = [
                w_down[:, pl.ds(pl.multiple_of(kv_at(place, i) * width, width), width)]
                for i in (j, j + 1)
            ]
            pair = dot(hidden, jnp.concatenate(weights, axis=1))
            for i in (j, j + 1):
                cols = slice((i - j) * width, (i - j + 1) * width)
                from_mine, from_other = pair[:half, cols], pair[half:, cols]
                keep[place][i] = jnp.where(own, from_mine, pltpu.roll(from_other, width // 2, 1))
                send[place][i] = jnp.where(
                    own, pltpu.roll(from_mine, width // 2, 1), from_other
                ).astype(BF16)


def result_kernel(parts, resid, out):
    half, width = resid.shape
    total = parts[0].astype(F32)
    for j in range(1, parts.shape[0]):
        total = total + parts[j].astype(F32)
    total = (resid[...] + total).T
    out[:, :half] = total[: width // 2].astype(BF16)
    out[:, half:] = total[width // 2 :].astype(BF16)


def per_device(
    tokens,
    gain_mix,
    gain_mlp,
    decay_rate,
    w_query,
    w_key,
    w_value,
    w_gate,
    w_mix,
    w_up,
    w_down,
    state,
):
    seqs, heads, key_width, value_width = state.shape
    rows, own_cols = tokens.shape
    half = rows // 2
    cols = 2 * own_cols
    peers = lax.axis_size(KV)
    model_width = cols * peers
    sizes = ring_sizes()
    count = peers // 4
    qkvg = sum(w.shape[1] for w in (w_query, w_key, w_value, w_gate))
    payload_width = qkvg + LANES
    tokens_t = tokens.T

    def inputs_body(*refs):
        inputs_kernel(*refs, sizes=sizes)

    sources = [
        pltpu.with_memory_space_constraint(x, pltpu.HBM)
        for x in (tokens_t, gain_mix.reshape(peers, cols), w_query, w_key, w_value, w_gate)
    ]
    *payload, both = kernel_call(
        inputs_body,
        [((rows // 4, payload_width), BF16)] * 4 + [((rows, cols), BF16)],
        swap_tp(tokens_t),
        *sources,
        hbm=range(1, 7),
        scratch=[
            *(pltpu.VMEM(s.shape, s.dtype) for s in sources),
            pltpu.VMEM((4, rows // 4, cols), F32),
            pltpu.SemaphoreType.DMA((len(sources),)),
        ],
    )
    parts = sum_at_owner([piece.reshape(count, seqs, payload_width) for piece in payload])
    rates = lax.dynamic_slice_in_dim(decay_rate, lax.axis_index("tp") * heads, heads)
    (decayed,) = kernel_call(
        decay_kernel,
        [((seqs * heads, key_width, value_width), F32)],
        state.reshape(seqs * heads, key_width, value_width),
        jnp.broadcast_to(rates[:, None], (heads, value_width)),
        flops=10**7,
        bytes_accessed=2**23,
    )

    def retention_body(*refs):
        retention_kernel(
            *refs, model_width=model_width, sizes=(seqs, heads, key_width, value_width)
        )

    new_state, heads_out = kernel_call(
        retention_body,
        [
            ((seqs * heads, key_width, value_width), F32),
            ((count, seqs, heads * value_width), BF16),
        ],
        parts,
        decayed,
        scratch=[pltpu.VMEM((seqs, heads * value_width), F32)],
    )

    def mix_body(*refs):
        mix_kernel(*refs, sizes=sizes)

    keep, send = kernel_call(
        mix_body,
        [((half, cols), BF16)] * 2,
        *(x.reshape(rows // 4, heads * value_width) for x in gathered(heads_out)),
        w_mix,
        scratch=[pltpu.VMEM((rows, cols), F32)],
    )
    (resid,) = kernel_call(
        resid_kernel, [((count, half, cols), BF16)], both, keep, swap_tp(send)
    )
    mine = gathered(resid)
    other = [swap_tp(x) for x in mine]

    def mixer_body(*refs):
        mixer_kernel(*refs, model_width=model_width, sizes=sizes)

    piece = (count, half, cols)
    *out, own_resid = kernel_call(
        mixer_body,
        [(piece, F32)] * 4 + [(piece, BF16)] * 4 + [((half, cols), F32)],
        *mine,
        *other,
        gain_mlp.reshape(peers, cols),
        w_up,
        w_down,
    )
    chip_sum = {}
    for place in (*PLACES, 0):
        chip_sum[place] = (out[place] + swap_tp(out[4 + place]).astype(F32)).astype(BF16)
    parts = sum_at_owner(chip_sum)
    (result_t,) = kernel_call(result_kernel, [((own_cols, rows), BF16)], parts, own_resid)
    return (result_t.T, new_state.reshape(state.shape))


def solution(mesh):
    torus = Mesh(
        mesh.devices.reshape(mesh.shape["dp"], 8, 4, mesh.shape["tp"]), ("dp", "kv_0", "kv_1", "tp")
    )
    return jax.shard_map(
        per_device,
        mesh=torus,
        in_specs=(
            P("dp", KV_TP),
            P(),
            P(),
            P(),
            P(KV, "tp"),
            P(KV, "tp"),
            P(KV, "tp"),
            P(KV, "tp"),
            P("tp", KV),
            P(None, KV_TP),
            P(KV_TP, None),
            P(DP_KV, "tp", None, None),
        ),
        out_specs=(P("dp", KV_TP), P(DP_KV, "tp", None, None)),
        check_vma=False,
    )
```

```python
import jax
import jax.numpy as jnp
from jax import lax
from jax.experimental import pallas as pl
from jax.experimental.pallas import tpu as pltpu
from jax.sharding import Mesh
from jax.sharding import PartitionSpec as P

KV = ("kv_0", "kv_1")
KV_TP = ("kv_0", "kv_1", "tp")
DP_KV = ("dp", "kv_0", "kv_1")

EPS = 1e-06
F32 = jnp.float32
BF16 = jnp.bfloat16
LANES = 128


def dot(a, b):
    return jnp.dot(a, b, preferred_element_type=F32)


def kernel_call(body, outs, *args, scratch=(), hbm=(), flops=0, bytes_accessed=0):
    vmem = pl.BlockSpec(memory_space=pltpu.VMEM)
    in_hbm = pl.BlockSpec(memory_space=pltpu.HBM)
    return pl.pallas_call(
        body,
        out_shape=[jax.ShapeDtypeStruct(*o) for o in outs],
        in_specs=[in_hbm if i in hbm else vmem for i in range(len(args))],
        out_specs=[vmem] * len(outs),
        scratch_shapes=list(scratch),
        compiler_params=pltpu.CompilerParams(vmem_limit_bytes=10 * 2**20),
        cost_estimate=pl.CostEstimate(
            flops=flops, bytes_accessed=bytes_accessed, transcendentals=0
        ),
    )(*args)


def swap_tp(x):
    return lax.ppermute(x, "tp", [(0, 1), (1, 0)])


def ring_sizes():
    return lax.axis_size("kv_0"), lax.axis_size("kv_1")


def own_class():
    return 2 * (lax.axis_index("kv_0") % 2) + lax.axis_index("kv_1") % 2


def members(z_size, x_size):
    return [(zr, xr) for zr in range(z_size // 2) for xr in range(x_size // 2)]


def member_kv(member, which, x_size):
    return (2 * member[0] + which // 2) * x_size + 2 * member[1] + which % 2


def class_groups():
    z_size, x_size = ring_sizes()
    return [
        [member_kv(m, c, x_size) * 2 + tp for m in members(z_size, x_size)]
        for tp in range(2)
        for c in range(4)
    ]


def to_neighbour(x, place):
    z_size, x_size = ring_sizes()

    def across(position, tp, size):
        return (position + (1 if position % 2 == tp else -1)) % size

    pairs = []
    for z in range(z_size):
        for x_ in range(x_size):
            for tp in range(2):
                to_z = across(z, tp, z_size) if place & 2 else z
                to_x = across(x_, tp, x_size) if place & 1 else x_
                pairs.append(((z * x_size + x_) * 2 + tp, (to_z * x_size + to_x) * 2 + tp))
    return lax.ppermute(x, KV_TP, pairs)


def in_class(x):
    return lax.all_to_all(x, KV_TP, 0, 0, axis_index_groups=class_groups(), tiled=True)


PLACES = (3, 1, 2)


def sum_in_square(parts):
    arrived = {place: to_neighbour(parts[place], place) for place in PLACES}
    total = parts[0].astype(F32)
    for place in PLACES:
        total = total + arrived[place].astype(F32)
    return total.astype(BF16)


def from_square(own):
    arrived = {place: to_neighbour(own, place) for place in PLACES}
    return [own, *(arrived[place] for place in (1, 2, 3))]


def fetch_kernel(*refs):
    count = len(refs) // 2
    sem = refs[-1]
    copies = [
        pltpu.make_async_copy(refs[i], refs[count + i], sem.at[i]) for i in range(count)
    ]
    for copy in copies:
        copy.start()
    for copy in copies:
        copy.wait()


def inputs_kernel(other, own, gain, w_query, w_key, w_value, w_gate, *rest, sizes):
    outs, both_out, by_class = rest[:4], rest[4], rest[5]
    tp = lax.axis_index("tp")
    kv = lax.axis_index(KV)
    first, second = own[...].astype(F32), other[...].astype(F32)
    both = jnp.where(
        tp == 0,
        jnp.concatenate([first, second], axis=0),
        jnp.concatenate([second, first], axis=0),
    ).T
    both_out[...] = both.astype(BF16)
    seqs = both.shape[0] // (sizes[0] * sizes[1])
    for c in range(4):
        kvs = [member_kv(m, c, sizes[1]) for m in members(*sizes)]
        by_class[c] = jnp.concatenate([both[i * seqs : (i + 1) * seqs] for i in kvs], axis=0)
    both = jnp.concatenate([by_class[own_class() ^ place] for place in range(4)], axis=0)
    squares = jnp.sum(both * both, axis=1, keepdims=True)
    high = squares.astype(BF16).astype(F32)
    low = squares - high
    lane = lax.broadcasted_iota(jnp.int32, (squares.shape[0], LANES), 1)
    scaled = (both * gain[pl.ds(kv, 1), :]).astype(BF16)
    start = 0
    for weight in (w_query, w_key, w_value, w_gate):
        width = weight.shape[1]
        product = dot(scaled, weight[...]).astype(BF16)
        for place, out in enumerate(outs):
            count = out.shape[0]
            out[:, start : start + width] = product[place * count : (place + 1) * count]
        start += width
    totals = jnp.where(lane == 0, high, jnp.where(lane == 1, low, 0.0)).astype(BF16)
    for place, out in enumerate(outs):
        count = out.shape[0]
        out[:, start : start + LANES] = totals[place * count : (place + 1) * count]


def decay_kernel(state, rates, out):
    heads = rates.shape[0]
    decay = jnp.exp(-rates[...])
    for i in range(out.shape[0]):
        h = i % heads
        out[i] = decay[h : h + 1, :] * state[i]


def retention_kernel(
    parts, decayed, heads_out, key_out, value_out, read_ref, *, model_width, sizes
):
    seqs, heads, key_width, value_width = sizes
    total = parts[0].astype(F32)
    for j in range(1, parts.shape[0]):
        total = total + parts[j].astype(F32)
    q_end = heads * key_width
    k_end = 2 * q_end
    v_end = k_end + heads * value_width
    g_end = v_end + heads * value_width
    row_total = total[:, g_end : g_end + 1] + total[:, g_end + 1 : g_end + 2]
    scale = lax.rsqrt(row_total / model_width + EPS)

    def rounded(x):
        return (x * scale).astype(BF16).astype(F32)

    query = rounded(total[:, :q_end])
    key = rounded(total[:, q_end:k_end]) * key_width ** (-0.5)
    value = rounded(total[:, k_end:v_end])
    gate = rounded(total[:, v_end:g_end])
    query_t = query.T
    key_out[...] = key.T
    value_out[...] = value
    for b in range(seqs):
        for h in range(heads):
            rows = slice(h * key_width, (h + 1) * key_width)
            cols = slice(h * value_width, (h + 1) * value_width)
            read_ref[b : b + 1, cols] = jnp.sum(
                query_t[rows, b : b + 1] * decayed[b * heads + h], axis=0, keepdims=True
            )
    for h in range(heads):
        rows = slice(h * key_width, (h + 1) * key_width)
        cols = slice(h * value_width, (h + 1) * value_width)
        match = jnp.sum(query[:, rows] * key[:, rows], axis=1, keepdims=True)
        read = read_ref[:, cols] + match * value[:, cols]
        read = read * lax.rsqrt(jnp.mean(read * read, axis=1, keepdims=True) + EPS)
        g = gate[:, cols]
        done = (g / (1.0 + jnp.exp(-g)) * read).astype(BF16)
        for j in range(heads_out.shape[0]):
            heads_out[j, :, cols] = done


def state_kernel(decayed, key_t, value, new_state):
    seqs, width = value.shape
    key_width, value_width = decayed.shape[1:]
    heads = width // value_width
    for b in range(seqs):
        for h in range(heads):
            rows = slice(h * key_width, (h + 1) * key_width)
            cols = slice(h * value_width, (h + 1) * value_width)
            new_state[b * heads + h] = (
                decayed[b * heads + h] + key_t[rows, b : b + 1] * value[b : b + 1, cols]
            )


def mix_kernel(*refs, sizes):
    heads, w_mix, keep, send, product = refs[:4], *refs[4:]
    tp = lax.axis_index("tp")
    seqs = heads[0].shape[0] // len(members(*sizes))
    for place in range(4):
        piece = dot(heads[place][...], w_mix[...])
        for i, m in enumerate(members(*sizes)):
            kv = member_kv(m, own_class() ^ place, sizes[1])
            product[pl.ds(pl.multiple_of(kv * seqs, seqs), seqs), :] = piece[
                i * seqs : (i + 1) * seqs
            ]
    half = keep.shape[0]
    keep[...] = product[pl.ds(pl.multiple_of(tp * half, half), half), :].astype(BF16)
    send[...] = product[pl.ds(pl.multiple_of((1 - tp) * half, half), half), :].astype(BF16)


def resid_kernel(both, keep, received, out):
    half = keep.shape[0]
    start = pl.multiple_of(lax.axis_index("tp") * half, half)
    mixed = keep[...].astype(F32) + received[...].astype(F32)
    resid = (both[pl.ds(start, half), :].astype(F32) + mixed).astype(BF16)
    for j in range(out.shape[0]):
        out[j] = resid


def up_kernel(mine, other, gain, w_up, upper, squares, *, place, sizes):
    count, half, width = mine.shape
    total = jnp.zeros((2 * half, w_up.shape[1]), F32)
    square = jnp.zeros((2 * half, width), F32)
    for j in range(0, count, 2):
        pieces, weights = [], []
        for i in (j, j + 1):
            kv = member_kv(members(*sizes)[i], own_class() ^ place, sizes[1])
            block = jnp.concatenate([mine[i], other[i]], axis=0).astype(F32)
            square = square + block * block
            pieces.append((block * gain[pl.ds(kv, 1), :]).astype(BF16))
            weights.append(w_up[pl.ds(pl.multiple_of(kv * width, width), width), :])
        total = total + dot(jnp.concatenate(pieces, axis=1), jnp.concatenate(weights, axis=0))
    upper[...] = total
    squares[...] = square


def hidden_of(refs, model_width):
    upper = sum(ref[...] for ref in refs[0::2])
    squares = sum(ref[...] for ref in refs[1::2])
    scale = lax.rsqrt(jnp.sum(squares, axis=1, keepdims=True) / model_width + EPS)
    upper = jnp.maximum(upper * scale, 0.0)
    return (upper * upper).astype(BF16)


def own_lanes(half, width):
    lane = lax.broadcasted_iota(jnp.int32, (half, width), 1)
    return jnp.where(lane < width // 2, 0, 1) == lax.axis_index("tp")


def down_kernel(hidden, w_down, keep, send, *, place, sizes):
    count, half, width = keep.shape
    own = own_lanes(half, width)
    for j in range(0, count, 2):
        weights = []
        for i in (j, j + 1):
            kv = member_kv(members(*sizes)[i], own_class() ^ place, sizes[1])
            weights.append(w_down[:, pl.ds(pl.multiple_of(kv * width, width), width)])
        pair = dot(hidden[...], jnp.concatenate(weights, axis=1))
        for i in (j, j + 1):
            cols = slice((i - j) * width, (i - j + 1) * width)
            from_mine, from_other = pair[:half, cols], pair[half:, cols]
            keep[i] = jnp.where(own, from_mine, pltpu.roll(from_other, width // 2, 1))
            send[i] = jnp.where(own, pltpu.roll(from_mine, width // 2, 1), from_other).astype(BF16)


def own_resid_kernel(mine, other, resid, *, sizes):
    half, width = resid.shape
    kv = lax.axis_index(KV)
    spot = (kv // sizes[1] // 2) * (sizes[1] // 2) + kv % sizes[1] // 2
    resid[...] = jnp.where(
        own_lanes(half, width),
        mine[spot].astype(F32),
        pltpu.roll(other[spot].astype(F32), width // 2, 1),
    )


def result_kernel(parts, resid, out):
    half, width = resid.shape
    total = parts[0].astype(F32)
    for j in range(1, parts.shape[0]):
        total = total + parts[j].astype(F32)
    total = (resid[...] + total).T
    out[:, :half] = total[: width // 2].astype(BF16)
    out[:, half:] = total[width // 2 :].astype(BF16)


def per_device(
    tokens,
    gain_mix,
    gain_mlp,
    decay_rate,
    w_query,
    w_key,
    w_value,
    w_gate,
    w_mix,
    w_up,
    w_down,
    state,
):
    seqs, heads, key_width, value_width = state.shape
    rows, own_cols = tokens.shape
    half = rows // 2
    cols = 2 * own_cols
    peers = lax.axis_size(KV)
    model_width = cols * peers
    sizes = ring_sizes()
    count = peers // 4
    qkvg = sum(w.shape[1] for w in (w_query, w_key, w_value, w_gate))
    payload_width = qkvg + LANES
    tokens_t = tokens.T

    def inputs_body(*refs):
        inputs_kernel(*refs, sizes=sizes)

    sources = [
        pltpu.with_memory_space_constraint(x, pltpu.HBM)
        for x in (tokens_t, gain_mix.reshape(peers, cols), w_query, w_key, w_value, w_gate)
    ]
    fetched = kernel_call(
        fetch_kernel,
        [(x.shape, x.dtype) for x in sources],
        *sources,
        hbm=range(len(sources)),
        scratch=[pltpu.SemaphoreType.DMA((len(sources),))],
        flops=10**7,
        bytes_accessed=2**21,
    )
    *payload, both = kernel_call(
        inputs_body,
        [((rows // 4, payload_width), BF16)] * 4 + [((rows, cols), BF16)],
        swap_tp(tokens_t),
        *fetched,
        scratch=[pltpu.VMEM((4, rows // 4, cols), F32)],
    )
    rates = lax.dynamic_slice_in_dim(decay_rate, lax.axis_index("tp") * heads, heads)
    (decayed,) = kernel_call(
        decay_kernel,
        [((seqs * heads, key_width, value_width), F32)],
        state.reshape(seqs * heads, key_width, value_width),
        jnp.broadcast_to(rates[:, None], (heads, value_width)),
        flops=3 * 10**7,
        bytes_accessed=2**23,
    )
    total = sum_in_square([piece.reshape(count, seqs, payload_width) for piece in payload])
    total, decayed = lax.optimization_barrier((total, decayed))
    parts = in_class(total)

    def retention_body(*refs):
        retention_kernel(
            *refs, model_width=model_width, sizes=(seqs, heads, key_width, value_width)
        )

    heads_out, key_t, value = kernel_call(
        retention_body,
        [
            ((count, seqs, heads * value_width), BF16),
            ((heads * key_width, seqs), F32),
            ((seqs, heads * value_width), F32),
        ],
        parts,
        decayed,
        scratch=[pltpu.VMEM((seqs, heads * value_width), F32)],
    )
    far_heads = in_class(heads_out)
    key_t, far_heads = lax.optimization_barrier((key_t, far_heads))
    (new_state,) = kernel_call(
        state_kernel,
        [((seqs * heads, key_width, value_width), F32)],
        decayed,
        key_t,
        value,
        flops=3 * 10**7,
        bytes_accessed=2**23,
    )

    def mix_body(*refs):
        mix_kernel(*refs, sizes=sizes)

    keep, send = kernel_call(
        mix_body,
        [((half, cols), BF16)] * 2,
        *(x.reshape(rows // 4, heads * value_width) for x in from_square(far_heads)),
        w_mix,
        scratch=[pltpu.VMEM((rows, cols), F32)],
    )
    (resid,) = kernel_call(
        resid_kernel, [((count, half, cols), BF16)], both, keep, swap_tp(send)
    )
    mine = from_square(in_class(resid))
    other = [swap_tp(x) for x in mine]
    gains = gain_mlp.reshape(peers, cols)
    ups = []
    for place in range(4):

        def up_body(*refs, place=place):
            up_kernel(*refs, place=place, sizes=sizes)

        ups += kernel_call(
            up_body,
            [((rows, w_up.shape[1]), F32), ((rows, cols), F32)],
            mine[place],
            other[place],
            gains,
            w_up,
            flops=10**7,
            bytes_accessed=2**21,
        )

    def resid_body(*refs):
        own_resid_kernel(*refs, sizes=sizes)

    (own_resid,) = kernel_call(
        resid_body, [((half, cols), F32)], mine[0], other[0], flops=10**5
    )
    piece = (count, half, cols)
    chip_sum = {}
    hidden = None
    for place in (*PLACES, 0):

        def down_body(*refs, place=place):
            down_kernel(*refs, place=place, sizes=sizes)

        def first_down_body(*refs, place=place):
            hidden_ref = refs[-1]
            hidden_ref[...] = hidden_of(refs[: len(ups)], model_width)
            down_kernel(hidden_ref, *refs[len(ups) : -1], place=place, sizes=sizes)

        outs = [(piece, F32), (piece, BF16)]
        if hidden is None:
            keep, send, hidden = kernel_call(
                first_down_body, [*outs, ((rows, w_up.shape[1]), BF16)], *ups, w_down
            )
        else:
            keep, send = kernel_call(
                down_body, outs, hidden, w_down, flops=10**7, bytes_accessed=2**21
            )
        chip_sum[place] = (keep + swap_tp(send).astype(F32)).astype(BF16)
    total, own_resid, new_state = lax.optimization_barrier(
        (sum_in_square(chip_sum), own_resid, new_state)
    )
    parts = in_class(total)
    (result_t,) = kernel_call(result_kernel, [((own_cols, rows), BF16)], parts, own_resid)
    return (result_t.T, new_state.reshape(state.shape))


def solution(mesh):
    torus = Mesh(
        mesh.devices.reshape(mesh.shape["dp"], 8, 4, mesh.shape["tp"]), ("dp", "kv_0", "kv_1", "tp")
    )
    return jax.shard_map(
        per_device,
        mesh=torus,
        in_specs=(
            P("dp", KV_TP),
            P(),
            P(),
            P(),
            P(KV, "tp"),
            P(KV, "tp"),
            P(KV, "tp"),
            P(KV, "tp"),
            P("tp", KV),
            P(None, KV_TP),
            P(KV_TP, None),
            P(DP_KV, "tp", None, None),
        ),
        out_specs=(P("dp", KV_TP), P(DP_KV, "tp", None, None)),
        check_vma=False,
    )
```

```python
import jax
import jax.numpy as jnp
from jax import lax
from jax.experimental import pallas as pl
from jax.experimental.pallas import tpu as pltpu
from jax.sharding import Mesh
from jax.sharding import PartitionSpec as P

KV = ("kv_0", "kv_1")
KV_TP = ("kv_0", "kv_1", "tp")
DP_KV = ("dp", "kv_0", "kv_1")

EPS = 1e-06
F32 = jnp.float32
BF16 = jnp.bfloat16
LANES = 128


def dot(a, b):
    return jnp.dot(a, b, preferred_element_type=F32)


def kernel_call(body, outs, *args, scratch=(), hbm=(), flops=0, bytes_accessed=0):
    vmem = pl.BlockSpec(memory_space=pltpu.VMEM)
    in_hbm = pl.BlockSpec(memory_space=pltpu.HBM)
    return pl.pallas_call(
        body,
        out_shape=[jax.ShapeDtypeStruct(*o) for o in outs],
        in_specs=[in_hbm if i in hbm else vmem for i in range(len(args))],
        out_specs=[vmem] * len(outs),
        scratch_shapes=list(scratch),
        compiler_params=pltpu.CompilerParams(vmem_limit_bytes=10 * 2**20),
        cost_estimate=pl.CostEstimate(
            flops=flops, bytes_accessed=bytes_accessed, transcendentals=0
        ),
    )(*args)


def swap_tp(x):
    return lax.ppermute(x, "tp", [(0, 1), (1, 0)])


def ring_sizes():
    return lax.axis_size("kv_0"), lax.axis_size("kv_1")


def own_class():
    return 2 * (lax.axis_index("kv_0") % 2) + lax.axis_index("kv_1") % 2


def members(z_size, x_size):
    return [(zr, xr) for zr in range(z_size // 2) for xr in range(x_size // 2)]


def member_kv(member, which, x_size):
    return (2 * member[0] + which // 2) * x_size + 2 * member[1] + which % 2


def class_groups():
    z_size, x_size = ring_sizes()
    return [
        [member_kv(m, c, x_size) * 2 + tp for m in members(z_size, x_size)]
        for tp in range(2)
        for c in range(4)
    ]


def to_neighbour(x, place, split=True):
    z_size, x_size = ring_sizes()

    def across(position, tp, size):
        return (position + (1 if position % 2 == tp * split else -1)) % size

    pairs = []
    for z in range(z_size):
        for x_ in range(x_size):
            for tp in range(2):
                to_z = across(z, tp, z_size) if place & 2 else z
                to_x = across(x_, tp, x_size) if place & 1 else x_
                pairs.append(((z * x_size + x_) * 2 + tp, (to_z * x_size + to_x) * 2 + tp))
    return lax.ppermute(x, KV_TP, pairs)


def in_class(x):
    return lax.all_to_all(x, KV_TP, 0, 0, axis_index_groups=class_groups(), tiled=True)


PLACES = (3, 1, 2)


def sum_in_square(parts):
    arrived = {}
    for place in PLACES:
        arrived[place] = to_neighbour(parts[place], place)
    total = parts[0].astype(F32)
    for place in PLACES:
        total = total + arrived[place].astype(F32)
    return total.astype(BF16)


def from_square(own):
    arrived = {place: to_neighbour(own, place) for place in PLACES}
    return [own, *(arrived[place] for place in (1, 2, 3))]


def fetch_kernel(*refs):
    count = len(refs) // 2
    sem = refs[-1]
    copies = [
        pltpu.make_async_copy(refs[i], refs[count + i], sem.at[i]) for i in range(count)
    ]
    for copy in copies:
        copy.start()
    for copy in copies:
        copy.wait()


def inputs_kernel(other, own, gain, w_query, w_key, w_value, w_gate, *rest, sizes):
    outs, tokens_out, by_class = rest[:4], rest[4], rest[5]
    tp = lax.axis_index("tp")
    kv = lax.axis_index(KV)
    first, second = own[...].astype(F32), other[...].astype(F32)
    both = jnp.where(
        tp == 0,
        jnp.concatenate([first, second], axis=0),
        jnp.concatenate([second, first], axis=0),
    ).T
    seqs = both.shape[0] // (sizes[0] * sizes[1])
    for c in range(4):
        kvs = [member_kv(m, c, sizes[1]) for m in members(*sizes)]
        by_class[c] = jnp.concatenate([both[i * seqs : (i + 1) * seqs] for i in kvs], axis=0)
    for place in range(4):
        tokens_out[place] = by_class[own_class() ^ place].astype(BF16)
    both = jnp.concatenate([by_class[own_class() ^ place] for place in range(4)], axis=0)
    squares = jnp.sum(both * both, axis=1, keepdims=True)
    high = squares.astype(BF16).astype(F32)
    low = squares - high
    lane = lax.broadcasted_iota(jnp.int32, (squares.shape[0], LANES), 1)
    scaled = (both * gain[pl.ds(kv, 1), :]).astype(BF16)
    start = 0
    for weight in (w_query, w_key, w_value, w_gate):
        width = weight.shape[1]
        product = dot(scaled, weight[...]).astype(BF16)
        for place, out in enumerate(outs):
            count = out.shape[0]
            out[:, start : start + width] = product[place * count : (place + 1) * count]
        start += width
    totals = jnp.where(lane == 0, high, jnp.where(lane == 1, low, 0.0)).astype(BF16)
    for place, out in enumerate(outs):
        count = out.shape[0]
        out[:, start : start + LANES] = totals[place * count : (place + 1) * count]


def decay_kernel(state, rates, out):
    heads = rates.shape[0]
    decay = jnp.exp(-rates[...])
    for i in range(out.shape[0]):
        h = i % heads
        out[i] = decay[h : h + 1, :] * state[i]


def retention_kernel(
    parts, decayed, heads_out, key_out, value_out, read_ref, *, model_width, sizes
):
    seqs, heads, key_width, value_width = sizes
    total = parts[0].astype(F32)
    for j in range(1, parts.shape[0]):
        total = total + parts[j].astype(F32)
    q_end = heads * key_width
    k_end = 2 * q_end
    v_end = k_end + heads * value_width
    g_end = v_end + heads * value_width
    row_total = total[:, g_end : g_end + 1] + total[:, g_end + 1 : g_end + 2]
    scale = lax.rsqrt(row_total / model_width + EPS)

    def rounded(x):
        return (x * scale).astype(BF16).astype(F32)

    query = rounded(total[:, :q_end])
    key = rounded(total[:, q_end:k_end]) * key_width ** (-0.5)
    value = rounded(total[:, k_end:v_end])
    gate = rounded(total[:, v_end:g_end])
    query_t = query.T
    key_out[...] = key.T
    value_out[...] = value
    for b in range(seqs):
        for h in range(heads):
            rows = slice(h * key_width, (h + 1) * key_width)
            cols = slice(h * value_width, (h + 1) * value_width)
            read_ref[b : b + 1, cols] = jnp.sum(
                query_t[rows, b : b + 1] * decayed[b * heads + h], axis=0, keepdims=True
            )
    for h in range(heads):
        rows = slice(h * key_width, (h + 1) * key_width)
        cols = slice(h * value_width, (h + 1) * value_width)
        match = jnp.sum(query[:, rows] * key[:, rows], axis=1, keepdims=True)
        read = read_ref[:, cols] + match * value[:, cols]
        read = read * lax.rsqrt(jnp.mean(read * read, axis=1, keepdims=True) + EPS)
        g = gate[:, cols]
        done = (g / (1.0 + jnp.exp(-g)) * read).astype(BF16)
        for j in range(heads_out.shape[0]):
            heads_out[j, :, cols] = done


def state_kernel(decayed, key_t, value, new_state):
    seqs, width = value.shape
    key_width, value_width = decayed.shape[1:]
    heads = width // value_width
    for b in range(seqs):
        for h in range(heads):
            rows = slice(h * key_width, (h + 1) * key_width)
            cols = slice(h * value_width, (h + 1) * value_width)
            new_state[b * heads + h] = (
                decayed[b * heads + h] + key_t[rows, b : b + 1] * value[b : b + 1, cols]
            )


def pack_kernel(w_mix, tokens, *packs):
    depth = w_mix.shape[0]
    for place, pack in enumerate(packs, 1):
        pack[:depth, :] = w_mix[...]
        pack[depth:, :] = tokens[place]


def copy_kernel(x, out):
    out[...] = x[0]


def mix_kernel(heads, w_mix, *rest):
    packs, (keep, send, product) = rest[:3], rest[3:]
    tp = lax.axis_index("tp")
    depth = w_mix.shape[0]
    half = keep.shape[1]
    weights = [w_mix[...], *(pack[:depth, :] for pack in packs)]
    width = w_mix.shape[1]
    for place in (0, 2):
        pair = dot(heads[...], jnp.concatenate(weights[place : place + 2], axis=1))
        product[own_class() ^ place] = pair[:, :width]
        product[own_class() ^ (place + 1)] = pair[:, width:]
    for c in range(4):
        keep[c] = product[c, pl.ds(pl.multiple_of(tp * half, half), half), :].astype(BF16)
        send[c] = product[c, pl.ds(pl.multiple_of((1 - tp) * half, half), half), :].astype(BF16)


def resid_kernel(tokens, *rest):
    packs, (keep, received, out) = rest[:3], rest[3:]
    half = keep.shape[1]
    depth = packs[0].shape[0] - 2 * half
    start = pl.multiple_of(lax.axis_index("tp") * half, half)
    for place in range(4):
        c = own_class() ^ place
        if place:
            own = packs[place - 1][pl.ds(depth + start, half), :]
        else:
            own = tokens[pl.ds(start, half), :]
        mixed = keep[c].astype(F32) + received[c].astype(F32)
        resid = (own.astype(F32) + mixed).astype(BF16)
        for j in range(out.shape[0]):
            out[j, c] = resid


def up_kernel(*refs, sizes, model_width):
    places = (len(refs) - 3) // 2
    mine, other, (gain, w_up, hidden) = refs[:places], refs[places : 2 * places], refs[-3:]
    _, classes, half, width = mine[0].shape
    pieces = [*mine, *other]
    total = jnp.zeros((len(pieces) * half, w_up.shape[1]), F32)
    square = jnp.zeros((len(pieces) * half, width), F32)
    for i, m in enumerate(members(*sizes)):
        for c in range(0, classes, 2):
            blocks, weights = [], []
            for which in (c, c + 1):
                kv = member_kv(m, which, sizes[1])
                block = jnp.concatenate([x[i, which] for x in pieces], axis=0).astype(F32)
                square = square + block * block
                blocks.append((block * gain[kv : kv + 1, :]).astype(BF16))
                weights.append(w_up[kv * width : (kv + 1) * width, :])
            total = total + dot(
                jnp.concatenate(blocks, axis=1), jnp.concatenate(weights, axis=0)
            )
    scale = lax.rsqrt(jnp.sum(square, axis=1, keepdims=True) / model_width + EPS)
    total = jnp.maximum(total * scale, 0.0)
    hidden[...] = (total * total).astype(BF16)


def hidden_in_order(first, second, out, first_places, second_places):
    rows = out.shape[0] // 8
    for ref, places in ((first, first_places), (second, second_places)):
        for owner in range(2):
            for i, place in enumerate(places):
                start = (owner * len(places) + i) * rows
                to = owner * 4 * rows + (own_class() ^ place) * rows
                out[pl.ds(pl.multiple_of(to, rows), rows), :] = ref[start : start + rows, :]


def own_lanes(half, width):
    lane = lax.broadcasted_iota(jnp.int32, (half, width), 1)
    return jnp.where(lane < width // 2, 0, 1) == lax.axis_index("tp")


def down_kernel(hidden, w_down, keep, send, *, place, sizes):
    count, half, width = keep.shape
    own = own_lanes(half, width)
    for j in range(0, count, 2):
        weights = []
        for i in (j, j + 1):
            kv = member_kv(members(*sizes)[i], own_class() ^ place, sizes[1])
            weights.append(w_down[:, pl.ds(pl.multiple_of(kv * width, width), width)])
        pair = dot(hidden[...], jnp.concatenate(weights, axis=1))
        for i in (j, j + 1):
            cols = slice((i - j) * width, (i - j + 1) * width)
            from_mine, from_other = pair[:half, cols], pair[half:, cols]
            keep[i] = jnp.where(own, from_mine, pltpu.roll(from_other, width // 2, 1))
            send[i] = jnp.where(own, pltpu.roll(from_mine, width // 2, 1), from_other).astype(BF16)


def own_resid_kernel(*refs, sizes):
    mine, other, resid = refs[:4], refs[4:8], refs[8]
    kv = lax.axis_index(KV)
    spot = (kv // sizes[1] // 2) * (sizes[1] // 2) + kv % sizes[1] // 2
    rows, width = mine[0].shape[2:]
    for place in range(4):
        to = (own_class() ^ place) * rows
        resid[pl.ds(pl.multiple_of(to, rows), rows), :] = jnp.where(
            own_lanes(rows, width),
            mine[place][spot, own_class()].astype(F32),
            pltpu.roll(other[place][spot, own_class()].astype(F32), width // 2, 1),
        )


def result_kernel(parts, resid, out, *, sizes):
    half, width = resid.shape
    total = parts[0].astype(F32)
    for j in range(1, parts.shape[0]):
        total = total + parts[j].astype(F32)
    total = resid[...] + total
    halves = (total, pltpu.roll(total, width // 2, 1))
    count = len(members(*sizes))
    seqs = half // (2 * count)
    blocks = {}
    for i, m in enumerate(members(*sizes)):
        for c in range(4):
            start = (c * (count // 2) + i % (count // 2)) * seqs
            blocks[member_kv(m, c, sizes[1])] = halves[i // (count // 2)][start : start + seqs]
    rows = jnp.concatenate([blocks[kv] for kv in range(len(blocks))], axis=0)
    out[...] = rows.T[: width // 2].astype(BF16)


def layer(
    tokens,
    gain_mix,
    gain_mlp,
    decay_rate,
    w_query,
    w_key,
    w_value,
    w_gate,
    w_mix,
    w_up,
    w_down,
    state,
):
    seqs, heads, key_width, value_width = state.shape
    rows, own_cols = tokens.shape
    half = rows // 2
    cols = 2 * own_cols
    peers = lax.axis_size(KV)
    model_width = cols * peers
    sizes = ring_sizes()
    count = peers // 4
    qkvg = sum(w.shape[1] for w in (w_query, w_key, w_value, w_gate))
    payload_width = qkvg + LANES
    tokens_t = tokens.T

    def inputs_body(*refs):
        inputs_kernel(*refs, sizes=sizes)

    sources = [
        pltpu.with_memory_space_constraint(x, pltpu.HBM)
        for x in (tokens_t, gain_mix.reshape(peers, cols), w_query, w_key, w_value, w_gate)
    ]
    depth = w_mix.shape[0]
    fetched = kernel_call(
        fetch_kernel,
        [(x.shape, x.dtype) for x in sources],
        *sources,
        hbm=range(len(sources)),
        scratch=[pltpu.SemaphoreType.DMA((len(sources),))],
        flops=10**7,
        bytes_accessed=2**21,
    )
    *payload, own_tokens = kernel_call(
        inputs_body,
        [((rows // 4, payload_width), BF16)] * 4 + [((4, rows // 4, cols), BF16)],
        swap_tp(tokens_t),
        *fetched,
        scratch=[pltpu.VMEM((4, rows // 4, cols), F32)],
    )
    rates = lax.dynamic_slice_in_dim(decay_rate, lax.axis_index("tp") * heads, heads)
    (decayed,) = kernel_call(
        decay_kernel,
        [((seqs * heads, key_width, value_width), F32)],
        state.reshape(seqs * heads, key_width, value_width),
        jnp.broadcast_to(rates[:, None], (heads, value_width)),
        flops=3 * 10**7,
        bytes_accessed=2**23,
    )
    total = sum_in_square([piece.reshape(count, seqs, payload_width) for piece in payload])
    total, decayed = lax.optimization_barrier((total, decayed))
    packs = kernel_call(
        pack_kernel,
        [((depth + rows // 4, cols), BF16)] * 3,
        w_mix,
        own_tokens,
        flops=10**6,
        bytes_accessed=2**21,
    )
    (own_piece,) = kernel_call(copy_kernel, [((rows // 4, cols), BF16)], own_tokens)
    near_packs = {}
    for place in PLACES:
        near_packs[place] = to_neighbour(packs[place - 1], place, split=False)
    packs = [near_packs[place] for place in (1, 2, 3)]
    parts = in_class(total)

    def retention_body(*refs):
        retention_kernel(
            *refs, model_width=model_width, sizes=(seqs, heads, key_width, value_width)
        )

    heads_out, key_t, value = kernel_call(
        retention_body,
        [
            ((count, seqs, heads * value_width), BF16),
            ((heads * key_width, seqs), F32),
            ((seqs, heads * value_width), F32),
        ],
        parts,
        decayed,
        scratch=[pltpu.VMEM((seqs, heads * value_width), F32)],
    )
    far_heads = in_class(heads_out)
    key_t, far_heads = lax.optimization_barrier((key_t, far_heads))
    (new_state,) = kernel_call(
        state_kernel,
        [((seqs * heads, key_width, value_width), F32)],
        decayed,
        key_t,
        value,
        flops=3 * 10**7,
        bytes_accessed=2**23,
    )

    quarter = (4, rows // 8, cols)
    keep, send = kernel_call(
        mix_kernel,
        [(quarter, BF16)] * 2,
        far_heads.reshape(rows // 4, heads * value_width),
        w_mix,
        *packs,
        scratch=[pltpu.VMEM((4, rows // 4, cols), F32)],
    )
    (resid,) = kernel_call(
        resid_kernel, [((count, *quarter), BF16)], own_piece, *packs, keep, swap_tp(send)
    )
    mine = from_square(in_class(resid))
    other = [swap_tp(x) for x in mine]
    gains = gain_mlp.reshape(peers, cols)

    def up_body(*refs):
        up_kernel(*refs, sizes=sizes, model_width=model_width)

    early, late = (0, 3), (1, 2)
    hiddens = []
    for places in (early, late):
        (hidden,) = kernel_call(
            up_body,
            [((2 * len(places) * rows // 8, w_up.shape[1]), BF16)],
            *(mine[place] for place in places),
            *(other[place] for place in places),
            gains,
            w_up,
            flops=10**7,
            bytes_accessed=2**21,
        )
        hiddens.append(hidden)

    def own_resid_body(*refs):
        own_resid_kernel(*refs, sizes=sizes)

    (own_resid,) = kernel_call(
        own_resid_body, [((half, cols), F32)], *mine, *other, flops=10**5
    )
    piece = (count, half, cols)
    chip_sum = {}
    hidden = None
    for place in (*PLACES, 0):

        def down_body(*refs, place=place):
            down_kernel(*refs, place=place, sizes=sizes)

        def first_down_body(*refs, place=place):
            hidden_ref = refs[-1]
            hidden_in_order(*refs[:2], hidden_ref, early, late)
            down_kernel(hidden_ref, *refs[2:-1], place=place, sizes=sizes)

        outs = [(piece, F32), (piece, BF16)]
        if hidden is None:
            keep, send, hidden = kernel_call(
                first_down_body, [*outs, ((rows, w_up.shape[1]), BF16)], *hiddens, w_down
            )
        else:
            keep, send = kernel_call(
                down_body, outs, hidden, w_down, flops=10**7, bytes_accessed=2**21
            )
        chip_sum[place] = (keep + swap_tp(send).astype(F32)).astype(BF16)
    total, own_resid, new_state = lax.optimization_barrier(
        (sum_in_square(chip_sum), own_resid, new_state)
    )
    parts = in_class(total)

    def result_body(*refs):
        result_kernel(*refs, sizes=sizes)

    (result_t,) = kernel_call(result_body, [((own_cols, rows), BF16)], parts, own_resid)
    return (result_t.T, new_state.reshape(state.shape))


def solution(mesh):
    torus = Mesh(
        mesh.devices.reshape(mesh.shape["dp"], 8, 4, mesh.shape["tp"]), ("dp", "kv_0", "kv_1", "tp")
    )
    return jax.shard_map(
        layer,
        mesh=torus,
        in_specs=(
            P("dp", KV_TP),
            P(),
            P(),
            P(),
            P(KV, "tp"),
            P(KV, "tp"),
            P(KV, "tp"),
            P(KV, "tp"),
            P("tp", KV),
            P(None, KV_TP),
            P(KV_TP, None),
            P(DP_KV, "tp", None, None),
        ),
        out_specs=(P("dp", KV_TP), P(DP_KV, "tp", None, None)),
        check_vma=False,
    )
```

```python
import jax
import jax.numpy as jnp
from jax import lax
from jax.experimental import pallas as pl
from jax.experimental.pallas import tpu as pltpu
from jax.sharding import Mesh
from jax.sharding import PartitionSpec as P

KV = ("kv_0", "kv_1")
KV_TP = ("kv_0", "kv_1", "tp")
DP_KV = ("dp", "kv_0", "kv_1")

EPS = 1e-06
F32 = jnp.float32
BF16 = jnp.bfloat16
LANES = 128


def dot(a, b):
    return jnp.dot(a, b, preferred_element_type=F32)


def kernel_call(body, outs, *args, scratch=(), hbm=(), flops=0, bytes_accessed=0):
    vmem = pl.BlockSpec(memory_space=pltpu.VMEM)
    in_hbm = pl.BlockSpec(memory_space=pltpu.HBM)
    return pl.pallas_call(
        body,
        out_shape=[jax.ShapeDtypeStruct(*o) for o in outs],
        in_specs=[in_hbm if i in hbm else vmem for i in range(len(args))],
        out_specs=[vmem] * len(outs),
        scratch_shapes=list(scratch),
        compiler_params=pltpu.CompilerParams(vmem_limit_bytes=10 * 2**20),
        cost_estimate=pl.CostEstimate(
            flops=flops, bytes_accessed=bytes_accessed, transcendentals=0
        ),
    )(*args)


def swap_tp(x):
    return lax.ppermute(x, "tp", [(0, 1), (1, 0)])


def ring_sizes():
    return lax.axis_size("kv_0"), lax.axis_size("kv_1")


def own_class():
    return 2 * (lax.axis_index("kv_0") % 2) + lax.axis_index("kv_1") % 2


def members(z_size, x_size):
    return [(zr, xr) for zr in range(z_size // 2) for xr in range(x_size // 2)]


def member_kv(member, which, x_size):
    return (2 * member[0] + which // 2) * x_size + 2 * member[1] + which % 2


def class_groups():
    z_size, x_size = ring_sizes()
    return [
        [member_kv(m, c, x_size) * 2 + tp for m in members(z_size, x_size)]
        for tp in range(2)
        for c in range(4)
    ]


def to_neighbour(x, place, split=True):
    z_size, x_size = ring_sizes()

    def across(position, tp, size):
        return (position + (1 if position % 2 == tp * split else -1)) % size

    pairs = []
    for z in range(z_size):
        for x_ in range(x_size):
            for tp in range(2):
                to_z = across(z, tp, z_size) if place & 2 else z
                to_x = across(x_, tp, x_size) if place & 1 else x_
                pairs.append(((z * x_size + x_) * 2 + tp, (to_z * x_size + to_x) * 2 + tp))
    return lax.ppermute(x, KV_TP, pairs)


def in_class(x):
    return lax.all_to_all(x, KV_TP, 0, 0, axis_index_groups=class_groups(), tiled=True)


PLACES = (3, 1, 2)


def sum_in_square(parts):
    arrived = {}
    for place in PLACES:
        arrived[place] = to_neighbour(parts[place], place)
    total = parts[0].astype(F32)
    for place in PLACES:
        total = total + arrived[place].astype(F32)
    return total.astype(BF16)


def from_square(own):
    arrived = {place: to_neighbour(own, place) for place in PLACES}
    return [own, *(arrived[place] for place in (1, 2, 3))]


def fetch_kernel(*refs):
    count = len(refs) // 2
    sem = refs[-1]
    copies = [
        pltpu.make_async_copy(refs[i], refs[count + i], sem.at[i]) for i in range(count)
    ]
    for copy in copies:
        copy.start()
    for copy in copies:
        copy.wait()


def inputs_kernel(other, own, gain, w_query, w_key, w_value, w_gate, *rest, sizes):
    outs, tokens_out, by_class = rest[:4], rest[4], rest[5]
    tp = lax.axis_index("tp")
    kv = lax.axis_index(KV)
    first, second = own[...].astype(F32), other[...].astype(F32)
    both = jnp.where(
        tp == 0,
        jnp.concatenate([first, second], axis=0),
        jnp.concatenate([second, first], axis=0),
    ).T
    seqs = both.shape[0] // (sizes[0] * sizes[1])
    for c in range(4):
        kvs = [member_kv(m, c, sizes[1]) for m in members(*sizes)]
        by_class[c] = jnp.concatenate([both[i * seqs : (i + 1) * seqs] for i in kvs], axis=0)
    for place in range(4):
        tokens_out[place] = by_class[own_class() ^ place].astype(BF16)
    both = jnp.concatenate([by_class[own_class() ^ place] for place in range(4)], axis=0)
    squares = jnp.sum(both * both, axis=1, keepdims=True)
    high = squares.astype(BF16).astype(F32)
    low = squares - high
    lane = lax.broadcasted_iota(jnp.int32, (squares.shape[0], LANES), 1)
    scaled = (both * gain[pl.ds(kv, 1), :]).astype(BF16)
    start = 0
    for weight in (w_query, w_key, w_value, w_gate):
        width = weight.shape[1]
        product = dot(scaled, weight[...]).astype(BF16)
        for place, out in enumerate(outs):
            count = out.shape[0]
            out[:, start : start + width] = product[place * count : (place + 1) * count]
        start += width
    totals = jnp.where(lane == 0, high, jnp.where(lane == 1, low, 0.0)).astype(BF16)
    for place, out in enumerate(outs):
        count = out.shape[0]
        out[:, start : start + LANES] = totals[place * count : (place + 1) * count]


def decay_kernel(state, rates, out):
    heads = rates.shape[0]
    decay = jnp.exp(-rates[...])
    for i in range(out.shape[0]):
        h = i % heads
        out[i] = decay[h : h + 1, :] * state[i]


def retention_kernel(
    parts, decayed, heads_out, key_out, value_out, read_ref, *, model_width, sizes
):
    seqs, heads, key_width, value_width = sizes
    total = parts[0].astype(F32)
    for j in range(1, parts.shape[0]):
        total = total + parts[j].astype(F32)
    q_end = heads * key_width
    k_end = 2 * q_end
    v_end = k_end + heads * value_width
    g_end = v_end + heads * value_width
    row_total = total[:, g_end : g_end + 1] + total[:, g_end + 1 : g_end + 2]
    scale = lax.rsqrt(row_total / model_width + EPS)

    def rounded(x):
        return (x * scale).astype(BF16).astype(F32)

    query = rounded(total[:, :q_end])
    key = rounded(total[:, q_end:k_end]) * key_width ** (-0.5)
    value = rounded(total[:, k_end:v_end])
    gate = rounded(total[:, v_end:g_end])
    query_t = query.T
    key_out[...] = key.T
    value_out[...] = value
    for b in range(seqs):
        for h in range(heads):
            rows = slice(h * key_width, (h + 1) * key_width)
            cols = slice(h * value_width, (h + 1) * value_width)
            read_ref[b : b + 1, cols] = jnp.sum(
                query_t[rows, b : b + 1] * decayed[b * heads + h], axis=0, keepdims=True
            )
    for h in range(heads):
        rows = slice(h * key_width, (h + 1) * key_width)
        cols = slice(h * value_width, (h + 1) * value_width)
        match = jnp.sum(query[:, rows] * key[:, rows], axis=1, keepdims=True)
        read = read_ref[:, cols] + match * value[:, cols]
        read = read * lax.rsqrt(jnp.mean(read * read, axis=1, keepdims=True) + EPS)
        g = gate[:, cols]
        done = (g / (1.0 + jnp.exp(-g)) * read).astype(BF16)
        for j in range(heads_out.shape[0]):
            heads_out[j, :, cols] = done


def state_kernel(decayed, key_t, value, new_state):
    seqs, width = value.shape
    key_width, value_width = decayed.shape[1:]
    heads = width // value_width
    for b in range(seqs):
        for h in range(heads):
            rows = slice(h * key_width, (h + 1) * key_width)
            cols = slice(h * value_width, (h + 1) * value_width)
            new_state[b * heads + h] = (
                decayed[b * heads + h] + key_t[rows, b : b + 1] * value[b : b + 1, cols]
            )


def pack_kernel(w_mix, tokens, *packs):
    depth = w_mix.shape[0]
    for place, pack in enumerate(packs, 1):
        pack[:depth, :] = w_mix[...]
        pack[depth:, :] = tokens[place]


def copy_kernel(x, out):
    out[...] = x[0]


def mix_kernel(heads, w_mix, *rest):
    packs, (keep, send, product) = rest[:3], rest[3:]
    tp = lax.axis_index("tp")
    depth = w_mix.shape[0]
    half = keep.shape[1]
    weights = [w_mix[...], *(pack[:depth, :] for pack in packs)]
    width = w_mix.shape[1]
    for place in (0, 2):
        pair = dot(heads[...], jnp.concatenate(weights[place : place + 2], axis=1))
        product[own_class() ^ place] = pair[:, :width]
        product[own_class() ^ (place + 1)] = pair[:, width:]
    for c in range(4):
        keep[c] = product[c, pl.ds(pl.multiple_of(tp * half, half), half), :].astype(BF16)
        send[c] = product[c, pl.ds(pl.multiple_of((1 - tp) * half, half), half), :].astype(BF16)


def resid_kernel(tokens, *rest):
    packs, (keep, received, out) = rest[:3], rest[3:]
    half = keep.shape[1]
    depth = packs[0].shape[0] - 2 * half
    start = pl.multiple_of(lax.axis_index("tp") * half, half)
    for place in range(4):
        c = own_class() ^ place
        if place:
            own = packs[place - 1][pl.ds(depth + start, half), :]
        else:
            own = tokens[pl.ds(start, half), :]
        mixed = keep[c].astype(F32) + received[c].astype(F32)
        resid = (own.astype(F32) + mixed).astype(BF16)
        for j in range(out.shape[0]):
            out[j, c] = resid


def up_kernel(*refs, sizes, model_width):
    places = (len(refs) - 3) // 2
    mine, other, (gain, w_up, hidden) = refs[:places], refs[places : 2 * places], refs[-3:]
    _, classes, half, width = mine[0].shape
    pieces = [*mine, *other]
    total = jnp.zeros((len(pieces) * half, w_up.shape[1]), F32)
    square = jnp.zeros((len(pieces) * half, width), F32)
    for i, m in enumerate(members(*sizes)):
        for c in range(0, classes, 2):
            blocks, weights = [], []
            for which in (c, c + 1):
                kv = member_kv(m, which, sizes[1])
                block = jnp.concatenate([x[i, which] for x in pieces], axis=0).astype(F32)
                square = square + block * block
                blocks.append((block * gain[kv : kv + 1, :]).astype(BF16))
                weights.append(w_up[kv * width : (kv + 1) * width, :])
            total = total + dot(
                jnp.concatenate(blocks, axis=1), jnp.concatenate(weights, axis=0)
            )
    scale = lax.rsqrt(jnp.sum(square, axis=1, keepdims=True) / model_width + EPS)
    total = jnp.maximum(total * scale, 0.0)
    hidden[...] = (total * total).astype(BF16)


def hidden_in_order(first, second, out, first_places, second_places):
    rows = out.shape[0] // 8
    for ref, places in ((first, first_places), (second, second_places)):
        for owner in range(2):
            for i, place in enumerate(places):
                start = (owner * len(places) + i) * rows
                to = owner * 4 * rows + (own_class() ^ place) * rows
                out[pl.ds(pl.multiple_of(to, rows), rows), :] = ref[start : start + rows, :]


def own_lanes(half, width):
    lane = lax.broadcasted_iota(jnp.int32, (half, width), 1)
    return jnp.where(lane < width // 2, 0, 1) == lax.axis_index("tp")


def down_kernel(hidden, w_down, keep, send, *, place, sizes):
    count, half, width = keep.shape
    own = own_lanes(half, width)
    for j in range(0, count, 2):
        weights = []
        for i in (j, j + 1):
            kv = member_kv(members(*sizes)[i], own_class() ^ place, sizes[1])
            weights.append(w_down[:, pl.ds(pl.multiple_of(kv * width, width), width)])
        pair = dot(hidden[...], jnp.concatenate(weights, axis=1))
        for i in (j, j + 1):
            cols = slice((i - j) * width, (i - j + 1) * width)
            from_mine, from_other = pair[:half, cols], pair[half:, cols]
            keep[i] = jnp.where(own, from_mine, pltpu.roll(from_other, width // 2, 1))
            send[i] = jnp.where(own, pltpu.roll(from_mine, width // 2, 1), from_other).astype(BF16)


def own_resid_kernel(*refs, sizes):
    mine, other, resid = refs[:4], refs[4:8], refs[8]
    kv = lax.axis_index(KV)
    spot = (kv // sizes[1] // 2) * (sizes[1] // 2) + kv % sizes[1] // 2
    rows, width = mine[0].shape[2:]
    for place in range(4):
        to = (own_class() ^ place) * rows
        resid[pl.ds(pl.multiple_of(to, rows), rows), :] = jnp.where(
            own_lanes(rows, width),
            mine[place][spot, own_class()].astype(F32),
            pltpu.roll(other[place][spot, own_class()].astype(F32), width // 2, 1),
        )


def result_kernel(parts, resid, out, *, sizes):
    half, width = resid.shape
    total = parts[0].astype(F32)
    for j in range(1, parts.shape[0]):
        total = total + parts[j].astype(F32)
    total = resid[...] + total
    halves = (total, pltpu.roll(total, width // 2, 1))
    count = len(members(*sizes))
    seqs = half // (2 * count)
    blocks = {}
    for i, m in enumerate(members(*sizes)):
        for c in range(4):
            start = (c * (count // 2) + i % (count // 2)) * seqs
            blocks[member_kv(m, c, sizes[1])] = halves[i // (count // 2)][start : start + seqs]
    rows = jnp.concatenate([blocks[kv] for kv in range(len(blocks))], axis=0)
    out[...] = rows.T[: width // 2].astype(BF16)


def layer(
    tokens,
    gain_mix,
    gain_mlp,
    decay_rate,
    w_query,
    w_key,
    w_value,
    w_gate,
    w_mix,
    w_up,
    w_down,
    state,
):
    seqs, heads, key_width, value_width = state.shape
    rows, own_cols = tokens.shape
    half = rows // 2
    cols = 2 * own_cols
    peers = lax.axis_size(KV)
    model_width = cols * peers
    sizes = ring_sizes()
    count = peers // 4
    qkvg = sum(w.shape[1] for w in (w_query, w_key, w_value, w_gate))
    payload_width = qkvg + LANES
    tokens_t = tokens.T

    def inputs_body(*refs):
        inputs_kernel(*refs, sizes=sizes)

    sources = [
        pltpu.with_memory_space_constraint(x, pltpu.HBM)
        for x in (tokens_t, gain_mix.reshape(peers, cols), w_query, w_key, w_value, w_gate)
    ]
    depth = w_mix.shape[0]
    fetched = kernel_call(
        fetch_kernel,
        [(x.shape, x.dtype) for x in sources],
        *sources,
        hbm=range(len(sources)),
        scratch=[pltpu.SemaphoreType.DMA((len(sources),))],
        flops=10**7,
        bytes_accessed=2**21,
    )
    *payload, own_tokens = kernel_call(
        inputs_body,
        [((rows // 4, payload_width), BF16)] * 4 + [((4, rows // 4, cols), BF16)],
        swap_tp(tokens_t),
        *fetched,
        scratch=[pltpu.VMEM((4, rows // 4, cols), F32)],
    )
    rates = lax.dynamic_slice_in_dim(decay_rate, lax.axis_index("tp") * heads, heads)
    (decayed,) = kernel_call(
        decay_kernel,
        [((seqs * heads, key_width, value_width), F32)],
        state.reshape(seqs * heads, key_width, value_width),
        jnp.broadcast_to(rates[:, None], (heads, value_width)),
        flops=3 * 10**7,
        bytes_accessed=2**23,
    )
    total = sum_in_square([piece.reshape(count, seqs, payload_width) for piece in payload])
    total, decayed = lax.optimization_barrier((total, decayed))
    packs = kernel_call(
        pack_kernel,
        [((depth + rows // 4, cols), BF16)] * 3,
        w_mix,
        own_tokens,
        flops=10**6,
        bytes_accessed=2**21,
    )
    (own_piece,) = kernel_call(copy_kernel, [((rows // 4, cols), BF16)], own_tokens)
    near_packs = {}
    for place in PLACES:
        near_packs[place] = to_neighbour(packs[place - 1], place, split=False)
    packs = [near_packs[place] for place in (1, 2, 3)]
    parts = in_class(total)

    def retention_body(*refs):
        retention_kernel(
            *refs, model_width=model_width, sizes=(seqs, heads, key_width, value_width)
        )

    heads_out, key_t, value = kernel_call(
        retention_body,
        [
            ((count, seqs, heads * value_width), BF16),
            ((heads * key_width, seqs), F32),
            ((seqs, heads * value_width), F32),
        ],
        parts,
        decayed,
        scratch=[pltpu.VMEM((seqs, heads * value_width), F32)],
    )
    far_heads = in_class(heads_out)
    key_t, far_heads = lax.optimization_barrier((key_t, far_heads))
    (new_state,) = kernel_call(
        state_kernel,
        [((seqs * heads, key_width, value_width), F32)],
        decayed,
        key_t,
        value,
        flops=3 * 10**7,
        bytes_accessed=2**23,
    )

    quarter = (4, rows // 8, cols)
    keep, send = kernel_call(
        mix_kernel,
        [(quarter, BF16)] * 2,
        far_heads.reshape(rows // 4, heads * value_width),
        w_mix,
        *packs,
        scratch=[pltpu.VMEM((4, rows // 4, cols), F32)],
    )
    (resid,) = kernel_call(
        resid_kernel, [((count, *quarter), BF16)], own_piece, *packs, keep, swap_tp(send)
    )
    mine = from_square(in_class(resid))
    other = [swap_tp(x) for x in mine]
    gains = gain_mlp.reshape(peers, cols)

    def up_body(*refs):
        up_kernel(*refs, sizes=sizes, model_width=model_width)

    early, late = (0, 3), (1, 2)
    hiddens = []
    for places in (early, late):
        (hidden,) = kernel_call(
            up_body,
            [((2 * len(places) * rows // 8, w_up.shape[1]), BF16)],
            *(mine[place] for place in places),
            *(other[place] for place in places),
            gains,
            w_up,
            flops=10**7,
            bytes_accessed=2**21,
        )
        hiddens.append(hidden)

    def own_resid_body(*refs):
        own_resid_kernel(*refs, sizes=sizes)

    (own_resid,) = kernel_call(
        own_resid_body, [((half, cols), F32)], *mine, *other, flops=10**5
    )
    piece = (count, half, cols)

    def first_down_body(*refs):
        hidden_ref = refs[-1]
        hidden_in_order(*refs[:2], hidden_ref, early, late)
        down_kernel(hidden_ref, *refs[2:-1], place=3, sizes=sizes)

    def pair_down_body(hidden_ref, weights, keep_ref, send_ref):
        for i, place in enumerate((1, 2)):
            down_kernel(
                hidden_ref, weights, keep_ref.at[i], send_ref.at[i], place=place, sizes=sizes
            )

    def own_down_body(*refs):
        down_kernel(*refs, place=0, sizes=sizes)

    def chip_total(keep, send):
        return (keep + swap_tp(send).astype(F32)).astype(BF16)

    keep, send, hidden = kernel_call(
        first_down_body,
        [(piece, F32), (piece, BF16), ((rows, w_up.shape[1]), BF16)],
        *hiddens,
        w_down,
    )
    chip_sum = {3: chip_total(keep, send)}
    keep, send = kernel_call(
        pair_down_body,
        [((2, *piece), F32), ((2, *piece), BF16)],
        hidden,
        w_down,
        flops=2 * 10**7,
        bytes_accessed=2**22,
    )
    received = swap_tp(send)
    for i, place in enumerate((1, 2)):
        chip_sum[place] = (keep[i] + received[i].astype(F32)).astype(BF16)
    keep, send = kernel_call(
        own_down_body,
        [(piece, F32), (piece, BF16)],
        hidden,
        w_down,
        flops=10**7,
        bytes_accessed=2**21,
    )
    chip_sum[0] = chip_total(keep, send)
    total, own_resid, new_state = lax.optimization_barrier(
        (sum_in_square(chip_sum), own_resid, new_state)
    )
    parts = in_class(total)

    def result_body(*refs):
        result_kernel(*refs, sizes=sizes)

    (result_t,) = kernel_call(result_body, [((own_cols, rows), BF16)], parts, own_resid)
    return (result_t.T, new_state.reshape(state.shape))


def solution(mesh):
    torus = Mesh(
        mesh.devices.reshape(mesh.shape["dp"], 8, 4, mesh.shape["tp"]), ("dp", "kv_0", "kv_1", "tp")
    )
    return jax.shard_map(
        layer,
        mesh=torus,
        in_specs=(
            P("dp", KV_TP),
            P(),
            P(),
            P(),
            P(KV, "tp"),
            P(KV, "tp"),
            P(KV, "tp"),
            P(KV, "tp"),
            P("tp", KV),
            P(None, KV_TP),
            P(KV_TP, None),
            P(DP_KV, "tp", None, None),
        ),
        out_specs=(P("dp", KV_TP), P(DP_KV, "tp", None, None)),
        check_vma=False,
    )
```
